32 devices in a mesh: sp: 8 (over z, y), tp: 4 (over x, core).
Axes of the slice: x: 2, y: 2, z: 4, core: 2. Of those that a mesh axis runs over, the one named last changes fastest.
Arguments:
- stream_in: bfloat16 [6144, 2048], P(('sp', 'tp')), may hold values from -6 to 6
- query_wide: bfloat16 [6144, 512], P('sp', 'tp'), may hold values from -6 to 6
- key_wide: bfloat16 [6144, 512], P('sp', 'tp'), may hold values from -6 to 6
- value_wide: bfloat16 [6144, 512], P('sp', 'tp'), may hold values from -6 to 6
- gate_wide: bfloat16 [6144, 512], P('sp', 'tp'), may hold values from -6 to 6
- decay_wide: float32 [4, 6144], P('tp', 'sp'), may hold values from -2.3 to 0, as said below
- query_narrow: bfloat16 [6144, 512], P('sp', 'tp'), may hold values from -6 to 6
- key_narrow: bfloat16 [6144, 512], P('sp', 'tp'), may hold values from -6 to 6
- value_narrow: bfloat16 [6144, 512], P('sp', 'tp'), may hold values from -6 to 6
- gate_narrow: bfloat16 [6144, 512], P('sp', 'tp'), may hold values from -6 to 6
- decay_narrow: float32 [8, 6144], P('tp', 'sp'), may hold values from -2.3 to 0, as said below
- output_wide: bfloat16 [512, 2048], P('tp'), may hold values from -0.25 to 0.25
- output_narrow: bfloat16 [512, 2048], P('tp'), may hold values from -0.25 to 0.25
- norm_gain: bfloat16 [2048], replicated, may hold values from 0.099609375 to 1.8984375
- up_weight: bfloat16 [2048, 8192], P('sp', 'tp'), may hold values from -0.125 to 0.125
- down_weight: bfloat16 [8192, 2048], P('tp', 'sp'), may hold values from -0.0625 to 0.0625
Outputs:
- layer_out: bfloat16 [6144, 2048], P(('sp', 'tp'))
The draws below stay inside these ranges and needn't reach their ends.
Inputs may be any that keep to these rules, and one draw needn't show every extreme that they name: `decay_wide`: each entry is the logarithm of one head's retention factor at one position. `decay_narrow`: each entry is the logarithm of one head's retention factor at one position.
All inputs are finite; a program needn't handle non-finite values.
Results may differ from the reference program's by a relative error of at most 0.02.
Values may be sent and summed in bfloat16 or wider, within the bound.
A program may use at most 128 MiB of HBM per device.

```python
import math
import jax
import jax.numpy as jnp
from jax import lax

D = 2048
FF = 8192
HEADS_W = 4
HEADS_N = 8
HDW = 128
HDN = 64
BLOCK = 128
TOK_DEV = 768
RW = 512
RN = 512
TOKEN_POSITIONS = 6144


spike_count = 3


def log_decay_table(key, count_of_heads, slow_share):
    random_subkey_list = jax.random.split(key, 6)
    slow_heads = jax.random.uniform(random_subkey_list[0], (count_of_heads,), jnp.float32) < slow_share
    slow_rate = jax.random.uniform(random_subkey_list[1], (count_of_heads,), jnp.float32, 0.15, 0.4) * math.log(10.0) / TOKEN_POSITIONS
    fast_rate = 1.0 / jax.random.uniform(random_subkey_list[2], (count_of_heads,), jnp.float32, 30.0, 100.0)
    decay_rate = jnp.where(slow_heads, slow_rate, fast_rate)
    stretch = jnp.exp(jax.random.uniform(random_subkey_list[3], (TOKEN_POSITIONS // TOK_DEV,), jnp.float32, -math.log(2.0), math.log(2.0)))
    stretch = jnp.repeat(stretch, TOK_DEV)
    logarithm_base = -decay_rate[:, None] * stretch[None, :]
    spike_locations = jax.random.randint(random_subkey_list[4], (spike_count,), 0, TOKEN_POSITIONS)
    spike_labels = (jnp.arange(TOKEN_POSITIONS)[None, :] == spike_locations[:, None]).astype(jnp.float32)
    spike_removals = jax.random.uniform(random_subkey_list[5], (count_of_heads, spike_count), jnp.float32, math.log(0.5), math.log(0.8))
    return logarithm_base + jnp.dot(spike_removals, spike_labels)


def draw_decay_wide(key, part):
    share = 0.5
    return log_decay_table(jax.random.fold_in(key, 11), HEADS_W, share)


def draw_decay_narrow(key, part):
    share = 0.5
    return log_decay_table(jax.random.fold_in(key, 23), HEADS_N, share)


def steps_of(own_key, extent, shards, least, largest):
    def one(position, blocks):
        draws = jax.random.uniform(jax.random.fold_in(jax.random.fold_in(own_key, 6), position), (blocks,), jnp.float32, least / len(shards), largest / len(shards))
        return jnp.repeat(jnp.exp(draws), extent[position] // blocks).reshape((-1,) + (1,) * (len(extent) - position - 1))

    level = one(*shards[0])
    for cut in shards[1:]:
        level = level * one(*cut)
    return level


def scatter_about(key, extent, scale, most, pieces=(), kind=jnp.bfloat16):
    loudness = steps_of(key, extent, pieces, -0.22, 0.18) if pieces else 1.0
    drawn = jax.random.normal(key, extent, jnp.float32) * scale * loudness
    return jnp.minimum(jnp.maximum(drawn, -most), most).astype(kind)


def setup_inputs(seed: int = 0) -> dict:
    splits = jax.random.split(jax.random.key(seed), 17)
    return {
        "stream_in": scatter_about(splits[0], (TOKEN_POSITIONS, D), 1.0, 6.0, ((0, 32),)),
        "query_wide": scatter_about(splits[1], (TOKEN_POSITIONS, RW), 1.0, 6.0, ((0, 8), (1, 4))),
        "key_wide": scatter_about(splits[2], (TOKEN_POSITIONS, RW), 1.0, 6.0, ((0, 8), (1, 4))),
        "value_wide": scatter_about(splits[3], (TOKEN_POSITIONS, RW), 1.0, 6.0, ((0, 8), (1, 4))),
        "gate_wide": scatter_about(splits[4], (TOKEN_POSITIONS, RW), 1.0, 6.0, ((0, 8), (1, 4))),
        "decay_wide": draw_decay_wide(jax.random.fold_in(splits[16], 71), 0),
        "query_narrow": scatter_about(splits[6], (TOKEN_POSITIONS, RN), 1.0, 6.0, ((0, 8), (1, 4))),
        "key_narrow": scatter_about(splits[7], (TOKEN_POSITIONS, RN), 1.0, 6.0, ((0, 8), (1, 4))),
        "value_narrow": scatter_about(splits[8], (TOKEN_POSITIONS, RN), 1.0, 6.0, ((0, 8), (1, 4))),
        "gate_narrow": scatter_about(splits[9], (TOKEN_POSITIONS, RN), 1.0, 6.0, ((0, 8), (1, 4))),
        "decay_narrow": draw_decay_narrow(jax.random.fold_in(splits[16], 71), 0),
        "output_wide": scatter_about(splits[11], (RW, D), RW ** -0.5, 0.25, ((0, 4),)),
        "output_narrow": scatter_about(splits[12], (RN, D), RN ** -0.5, 0.25, ((0, 4),)),
        "norm_gain": jnp.clip(1.0 + 0.18 * jax.random.normal(splits[13], (D,), jnp.float32), 0.099609375, 1.8984375).astype(jnp.bfloat16),
        "up_weight": scatter_about(splits[14], (D, FF), D ** -0.5, 0.125, ((0, 8), (1, 4))),
        "down_weight": scatter_about(splits[15], (FF, D), FF ** -0.5, 0.0625, ((0, 4), (1, 8))),
    }


head_eps = 1e-05
norm_eps = 1e-06
rope_base = 10000.0

def rotate(values, places):
    half = values.shape[-1] // 2
    inverse = rope_base ** (-jnp.arange(half, dtype=jnp.float32) / half)
    angles = places[:, None] * inverse[None, :]
    cosine = jnp.cos(angles)[:, None, :]
    sine = jnp.sin(angles)[:, None, :]
    front = values[..., :half]
    back = values[..., half:]
    return jnp.concatenate([front * cosine - back * sine, back * cosine + front * sine], axis=-1)

def block_step(carried, inputs):
    query, keys, values, log_rate = inputs
    running = jnp.cumsum(log_rate, axis=0)
    spread = running[:, None, :] - running[None, :, :]
    length = log_rate.shape[0]
    lower = (jnp.arange(length)[:, None] >= jnp.arange(length)[None, :])[:, :, None]
    factor = jnp.where(lower, jnp.exp(jnp.minimum(spread, 0.0)), 0.0)
    scores = jnp.einsum('thd,shd->tsh', query, keys) * factor
    within = jnp.einsum('tsh,she->the', scores, values)
    across = jnp.einsum('thd,hde->the', query, carried) * jnp.exp(running)[:, :, None]
    tail_decay = jnp.exp(running[-1][None, :] - running)
    updated = jnp.exp(running[-1])[:, None, None] * carried + jnp.einsum('shd,she->hde', keys * tail_decay[:, :, None], values)
    return (updated, within + across)

def retain(query, keys, values, log_rate):
    length, count_of_heads, width = query.shape
    blocks = length // BLOCK

    def shaped(array):
        return array.reshape(blocks, BLOCK, count_of_heads, width)
    rates = log_rate.T.reshape(blocks, BLOCK, count_of_heads)
    carried = jnp.zeros((count_of_heads, width, width), jnp.float32)
    final_state, outputs = lax.scan(block_step, carried, (shaped(query), shaped(keys), shaped(values), rates))
    return outputs.reshape(length, count_of_heads, width)

def head_norm(values):
    centre = values - lax.optimization_barrier(jnp.mean(values, axis=-1, keepdims=True))
    spread = lax.optimization_barrier(jnp.mean(centre * centre, axis=-1, keepdims=True))
    return centre * lax.rsqrt(spread + head_eps)

def group(query, keys, values, gate, log_rate, width, places):
    length = query.shape[0]
    count_of_heads = query.shape[1] // width

    def split(array):
        return array.astype(jnp.float32).reshape(length, count_of_heads, width)
    query_rot = rotate(split(query), places)
    keys_rot = rotate(split(keys), places) * width ** (-0.5)
    normed = head_norm(retain(query_rot, keys_rot, split(values), log_rate)).reshape(length, count_of_heads * width)
    return (jax.nn.silu(gate.astype(jnp.float32)) * normed).astype(jnp.bfloat16)

def reference(stream_in, query_wide, key_wide, value_wide, gate_wide, decay_wide, query_narrow, key_narrow, value_narrow, gate_narrow, decay_narrow, output_wide, output_narrow, norm_gain, up_weight, down_weight):
    places = jnp.arange(TOKEN_POSITIONS, dtype=jnp.float32)
    mixed_wide = group(query_wide, key_wide, value_wide, gate_wide, decay_wide, HDW, places)
    mixed_narrow = group(query_narrow, key_narrow, value_narrow, gate_narrow, decay_narrow, HDN, places)
    mixed_sum = jnp.dot(mixed_wide, output_wide, preferred_element_type=jnp.float32) + jnp.dot(mixed_narrow, output_narrow, preferred_element_type=jnp.float32)
    middle = (stream_in.astype(jnp.float32) + mixed_sum).astype(jnp.bfloat16)
    middle_f = middle.astype(jnp.float32)
    normed_rows = (middle_f * lax.rsqrt(lax.optimization_barrier(jnp.mean(middle_f * middle_f, axis=-1, keepdims=True)) + norm_eps) * norm_gain.astype(jnp.float32)).astype(jnp.bfloat16)
    up_sum = jnp.dot(normed_rows, up_weight, preferred_element_type=jnp.float32)
    hidden = jnp.square(jax.nn.relu(up_sum)).astype(jnp.bfloat16)
    down_sum = jnp.dot(hidden, down_weight, preferred_element_type=jnp.float32)
    return (middle_f + down_sum).astype(jnp.bfloat16)
```

```python
import functools
import jax
import jax.numpy as jnp
import numpy as np
from jax import lax
from jax.experimental import pallas as pl
from jax.experimental.pallas import tpu as pltpu
from jax.sharding import PartitionSpec as P

HDW = 128
HDN = 64
BLOCK = 128


head_eps = 1e-05
norm_eps = 1e-06
rope_base = 10000.0


def carried_in(shard, axis, join, neutral):
    place = lax.axis_index(axis)
    gathered = jax.tree.map(
        lambda a, kind: lax.all_gather(a.astype(kind), axis),
        shard,
        (jnp.bfloat16, jnp.bfloat16, jnp.bfloat16, jnp.bfloat16),
    )
    state = jax.tree.map(lambda a, e: jnp.zeros_like(a) + jnp.asarray(e, a.dtype), shard, neutral)

    def one(turn, state):
        return join(
            state,
            jax.tree.map(
                lambda a, own: lax.dynamic_index_in_dim(a, turn, 0, False).astype(own.dtype),
                gathered,
                shard,
            ),
        )

    return lax.fori_loop(0, place, one, state)


def rotate(values, places):
    half = values.shape[-1] // 2
    inverse = rope_base ** (-jnp.arange(half, dtype=jnp.float32) / half)
    angles = places[:, None] * inverse[None, :]
    cosine = jnp.cos(angles)[:, None, :]
    sine = jnp.sin(angles)[:, None, :]
    front = values[..., :half]
    back = values[..., half:]
    return jnp.concatenate([front * cosine - back * sine, back * cosine + front * sine], axis=-1)


def block_step(carried, inputs):
    query, keys, values, log_rate = inputs
    running = jnp.cumsum(log_rate, axis=0)
    spread = running[:, None, :] - running[None, :, :]
    length = log_rate.shape[0]
    lower = (jnp.arange(length)[:, None] >= jnp.arange(length)[None, :])[:, :, None]
    factor = jnp.where(lower, jnp.exp(jnp.minimum(spread, 0.0)), 0.0)
    scores = jnp.einsum("thd,shd->tsh", query, keys) * factor
    within = jnp.einsum("tsh,she->the", scores, values)
    across = jnp.einsum("thd,hde->the", query, carried) * jnp.exp(running)[:, :, None]
    tail_decay = jnp.exp(running[-1][None, :] - running)
    updated = jnp.exp(running[-1])[:, None, None] * carried + jnp.einsum(
        "shd,she->hde", keys * tail_decay[:, :, None], values
    )
    return (updated, within + across)


def head_norm(values):
    centre = values - jnp.mean(values, axis=-1, keepdims=True)
    spread = jnp.mean(centre * centre, axis=-1, keepdims=True)
    return centre * lax.rsqrt(spread + head_eps)


def local_group(query, keys, values, log_rate, width, places):
    length = query.shape[0]
    count_of_heads = query.shape[1] // width
    blocks = length // BLOCK

    def split(array):
        return array.astype(jnp.float32).reshape(length, count_of_heads, width)

    query_rot = rotate(split(query), places)
    keys_rot = rotate(split(keys), places) * width ** (-0.5)
    rates = log_rate.T
    carried = jnp.zeros((count_of_heads, width, width), jnp.float32)
    final_state, outputs = lax.scan(
        block_step,
        carried,
        (
            query_rot.reshape(blocks, BLOCK, count_of_heads, width),
            keys_rot.reshape(blocks, BLOCK, count_of_heads, width),
            split(values).reshape(blocks, BLOCK, count_of_heads, width),
            rates.reshape(blocks, BLOCK, count_of_heads),
        ),
    )
    running = jnp.cumsum(rates, axis=0)
    return (
        query_rot,
        outputs.reshape(length, count_of_heads, width),
        final_state,
        jnp.exp(running[-1]),
        running,
    )


def finish_group(query_rot, outputs, incoming, running, gate):
    length = outputs.shape[0]
    outputs = (
        outputs + jnp.einsum("thd,hde->the", query_rot, incoming) * jnp.exp(running)[:, :, None]
    )
    normed = head_norm(outputs).reshape(length, -1)
    return (jax.nn.silu(gate.astype(jnp.float32)) * normed).astype(jnp.bfloat16)


def chain(earlier, later):
    rate_wide, memory_wide, rate_narrow, memory_narrow = earlier
    later_rate_wide, later_memory_wide, later_rate_narrow, later_memory_narrow = later
    return (
        rate_wide * later_rate_wide,
        memory_wide * later_rate_wide[:, None, None] + later_memory_wide,
        rate_narrow * later_rate_narrow,
        memory_narrow * later_rate_narrow[:, None, None] + later_memory_narrow,
    )


def row_norm(middle, norm_gain):
    middle_f = middle.astype(jnp.float32)
    scale = lax.rsqrt(jnp.mean(middle_f * middle_f, axis=-1, keepdims=True) + norm_eps)
    return (middle_f * scale * norm_gain.astype(jnp.float32)).astype(jnp.bfloat16)


def on_device(
    stream_in,
    query_wide,
    key_wide,
    value_wide,
    gate_wide,
    decay_wide,
    query_narrow,
    key_narrow,
    value_narrow,
    gate_narrow,
    decay_narrow,
    output_wide,
    output_narrow,
    norm_gain,
    up_weight,
    down_weight,
):
    length = query_wide.shape[0]
    places = (lax.axis_index("sp") * length + jnp.arange(length, dtype=jnp.int32)).astype(
        jnp.float32
    )
    wide_query, wide_out, wide_state, wide_total, wide_running = local_group(
        query_wide, key_wide, value_wide, decay_wide, HDW, places
    )
    narrow_query, narrow_out, narrow_state, narrow_total, narrow_running = local_group(
        query_narrow, key_narrow, value_narrow, decay_narrow, HDN, places
    )
    identity = (
        jnp.ones_like(wide_total),
        jnp.zeros_like(wide_state),
        jnp.ones_like(narrow_total),
        jnp.zeros_like(narrow_state),
    )
    incoming = carried_in(
        (wide_total, wide_state, narrow_total, narrow_state), "sp", chain, identity
    )
    mixed_wide = finish_group(wide_query, wide_out, incoming[1], wide_running, gate_wide)
    mixed_narrow = finish_group(narrow_query, narrow_out, incoming[3], narrow_running, gate_narrow)
    mixed_sum = lax.psum_scatter(
        (
            jnp.dot(mixed_wide, output_wide, preferred_element_type=jnp.float32)
            + jnp.dot(mixed_narrow, output_narrow, preferred_element_type=jnp.float32)
        ).astype(jnp.bfloat16),
        "tp",
        scatter_dimension=0,
        tiled=True,
    ).astype(jnp.float32)
    middle = (stream_in.astype(jnp.float32) + mixed_sum).astype(jnp.bfloat16)
    normed = lax.all_gather(row_norm(middle, norm_gain), "tp", axis=0, tiled=True)
    up_sum = jnp.dot(
        normed,
        lax.all_gather(up_weight, "sp", axis=0, tiled=True),
        preferred_element_type=jnp.float32,
    )
    hidden = jnp.square(jax.nn.relu(up_sum)).astype(jnp.bfloat16)
    down_sum = jnp.dot(
        hidden,
        lax.all_gather(down_weight, "sp", axis=1, tiled=True),
        preferred_element_type=jnp.float32,
    )
    down_rows = lax.psum_scatter(
        down_sum.astype(jnp.bfloat16), "tp", scatter_dimension=0, tiled=True
    ).astype(jnp.float32)
    return (middle.astype(jnp.float32) + down_rows).astype(jnp.bfloat16)


F32 = jnp.float32
BF16 = jnp.bfloat16
MESH_ID = pl.DeviceIdType.MESH


def turn_tables(shards, length):
    lane = np.arange(128)
    offsets, starts = [], []
    for width in (HDW, HDN):
        half = width // 2
        inverse = rope_base ** (-((lane % half).astype(np.float64)) / half)
        inside = np.arange(BLOCK)[:, None] * inverse[None, :]
        first = (np.arange(shards * length // BLOCK) * BLOCK)[:, None] * inverse[None, :]
        offsets += [np.cos(inside), np.sin(inside)]
        starts += [np.cos(first), np.sin(first)]
    return np.stack(offsets).astype(np.float32), np.stack(starts).astype(np.float32)


def dot(a, b):
    return jnp.dot(a, b, preferred_element_type=F32)


def dot_rows(a, b):
    return lax.dot_general(a, b, (((0,), (0,)), ((), ())), preferred_element_type=F32)


def dot_cols(a, b):
    return lax.dot_general(a, b, (((1,), (1,)), ((), ())), preferred_element_type=F32)


def layer_kernel(
    SP, TP,
    stream, qw, kw, vw, gw, qn, kn, vn, gn, decay, offs, starts, gain, ow_w, ow_n, up, down,
    out,
    up_buf, down_buf, ow_buf, st_buf, k_rot, before, inside, mixed, mix_in, mid, rows, hidden, part,
    mate_in, x_in, y_in, last_in, z_in,
    ssem, rsem, lsem, zsend, zrecv, srecv,
):
    sp = lax.axis_index("sp")
    tp = lax.axis_index("tp")
    NZ = SP // 2
    z, y = sp // 2, sp % 2
    x, c = tp // 2, tp % 2
    T = qw.shape[0]
    NB = T // BLOCK
    RT = T // TP
    RH = RT // 2
    RB = up.shape[0]
    CB = down.shape[1]
    D = stream.shape[1]
    FH = up.shape[1] // 2
    heavy = (z == 1) | (z == 2)
    is_end = jnp.logical_not(heavy)
    pz = z + 1 - 2 * (z % 2)
    mz = NZ - 1 - z
    goal_z = jnp.where(heavy, mz, pz)

    def dev(zz, dy=0, dx=0, dc=0):
        return (zz * 2 + (y + dy) % 2, (x + dx) % 2 * 2 + (c + dc) % 2)

    x_dev, y_dev, mate_dev = dev(z, 0, 1), dev(z, 1), dev(z, 0, 0, 1)
    count = [0]
    pending = []

    def link():
        count[0] += 1
        return count[0] - 1

    def copy_of(k, src, dst, device):
        return pltpu.make_async_remote_copy(
            src_ref=src, dst_ref=dst, send_sem=ssem.at[k], recv_sem=rsem.at[k],
            device_id=device, device_id_type=MESH_ID,
        )

    def start(k, src, dst, device):
        copy = copy_of(k, src, dst, device)
        copy.start()
        pending.append(copy)
        return copy

    def send(src, dst, device):
        return start(link(), src, dst, device)

    def arrive(k, dst):
        copy_of(k, dst, dst, mate_dev).wait_recv()

    barrier = pltpu.get_barrier_semaphore()
    for d in range(1, NZ):
        pl.semaphore_signal(barrier, inc=1, device_id=dev((z + d) % NZ), device_id_type=MESH_ID)
    for device in (x_dev, y_dev, mate_dev, dev(z, 0, 1, 1)):
        pl.semaphore_signal(barrier, inc=1, device_id=device, device_id_type=MESH_ID)
    pl.semaphore_wait(barrier, NZ + 3)

    locals_ = []

    def keep(src, dst):
        copy = pltpu.make_async_copy(src, dst, lsem.at[len(locals_)])
        copy.start()
        locals_.append(copy)
        return copy

    HB = RB // 2
    HF = FH // 2

    def up_at(zs, yy, part_of):
        return up_buf.at[pl.ds(pl.multiple_of((zs * 2 + yy) * RB + part_of * HB, HB), HB), :]

    def down_at(zs, yy):
        return down_buf.at[zs * 2 + yy]

    def up_half(half, part_of):
        return up.at[pl.ds(part_of * HB, HB), pl.ds(pl.multiple_of(half * FH, FH), FH)]

    def down_half(half, part_of):
        return down.at[pl.ds(pl.multiple_of(half * FH + part_of * HF, HF), HF), :]

    z_copies = []

    def z_copy(slot, sem, src, dst, zz):
        return pltpu.make_async_remote_copy(
            src_ref=src, dst_ref=dst, send_sem=zsend.at[slot], recv_sem=zrecv.at[sem],
            device_id=dev(zz), device_id_type=MESH_ID,
        )

    def up_sem(zs, yy, part_of):
        return (zs * 2 + yy) * 2 + part_of

    def down_sem(zs, yy):
        return 4 * NZ + zs * 2 + yy

    z_slots = [0]

    def z_slot():
        z_slots[0] += 1
        return z_slots[0] - 1

    def up_send(zs, yy, part_of, src, zz, into):
        copy = z_copy(z_slot(), up_sem(zs, yy, part_of), src, up_at(zs, yy, part_of), zz)
        copy.start()
        into.append(copy)

    def down_send(zs, yy, src, zz, into):
        copy = z_copy(z_slot(), down_sem(zs, yy), src, down_at(zs, yy), zz)
        copy.start()
        into.append(copy)

    def up_wait(zs, yy, part_of):
        ref = up_at(zs, yy, part_of)
        z_copy(0, up_sem(zs, yy, part_of), ref, ref, goal_z).wait_recv()

    def down_wait(zs, yy):
        ref = down_at(zs, yy)
        z_copy(0, down_sem(zs, yy), ref, ref, goal_z).wait_recv()

    oy = 1 - y
    ox = 1 - x
    SW = D // 4

    def ow_at(i, g, cols):
        return ow_buf.at[i, pl.ds(g * 128, 128), cols]

    def relay_cols(yy):
        return pl.ds(pl.multiple_of(yy * 3 * SW, SW), SW)

    main_cols = pl.ds(SW, 2 * SW)
    every = pl.ds(0, D)
    side = ox * 2 + c
    ow_first = [
        send(r.at[:, relay_cols(y)], ow_at(tp, g, relay_cols(y)), x_dev) for g, r in enumerate((ow_w, ow_n))
    ]
    ow_main = [
        send(r.at[:, main_cols], ow_at(tp, g, main_cols), x_dev) for g, r in enumerate((ow_w, ow_n))
    ]
    ow_mate = [send(r, ow_at(tp, g, every), mate_dev) for g, r in enumerate((ow_w, ow_n))]
    up_send(z, y, 0, up_half(y, 0), goal_z, z_copies)
    keep(ow_w, ow_at(tp, 0, every))
    keep(ow_n, ow_at(tp, 1, every))
    keep(up_half(y, 0), up_at(z, y, 0))
    keep(up_half(y, 1), up_at(z, y, 1))
    down_kept = [
        keep(down_half(y, i), down_buf.at[sp, pl.ds(i * HF, HF), :]) for i in range(2)
    ]

    lane = lax.broadcasted_iota(jnp.int32, (128, 128), 1)
    row = lax.broadcasted_iota(jnp.int32, (128, 128), 0)
    lower = row >= lane
    low = lane < HDN
    low_row = row < HDN
    low_half = lax.broadcasted_iota(jnp.int32, (HDN, 128), 1) < HDN
    diagonal = low == low_row
    cr = decay[...]
    step = 1
    while step < 128:
        cr = cr + jnp.where(lane >= step, pltpu.roll(cr, step, 1), 0.0)
        step *= 2
    ct = cr.T

    def col(h, b):
        return ct[:, h * NB + b:h * NB + b + 1]

    def line(h, b):
        return cr[h * NB + b:h * NB + b + 1, :]

    def total(h, b):
        return cr[h * NB + b:h * NB + b + 1, 127:128]

    def pair(a, b):
        return jnp.where(low, a, b)

    sign_w = jnp.where(low, -1.0, 1.0)
    early = (lane % HDN) < HDN // 2
    sign_n = jnp.where(early, -1.0, 1.0)

    def tables(g, b):
        cb = starts[2 * g, pl.ds(sp * NB + b, 1), :]
        sb = starts[2 * g + 1, pl.ds(sp * NB + b, 1), :]
        co, so = offs[2 * g], offs[2 * g + 1]
        return co * cb - so * sb, (so * cb + co * sb) * (sign_n if g else sign_w)

    def turned(v, table, g):
        if g:
            other = jnp.where(early, pltpu.roll(v, 128 - HDN // 2, 1), pltpu.roll(v, HDN // 2, 1))
        else:
            other = pltpu.roll(v, HDW // 2, 1)
        return v * table[0] + other * table[1]

    state_w = jnp.zeros((128, 128), F32)
    state_n = jnp.zeros((128, 128), F32)
    sums = [jnp.zeros((1, 1), F32) for _ in range(3)]
    for b in range(NB):
        rs = pl.ds(b * BLOCK, BLOCK)
        before[0, b] = state_w
        before[1, b] = state_n
        kwr = turned(kw[rs, :].astype(F32), tables(0, b), 0) * HDW ** (-0.5)
        knr = turned(kn[rs, :].astype(F32), tables(1, b), 1) * HDN ** (-0.5)
        k_rot[rs, 0:128] = kwr.astype(BF16)
        k_rot[rs, 128:256] = knr.astype(BF16)
        t0, t1, t2 = total(0, b), total(1, b), total(2, b)
        sums = [s + t for s, t in zip(sums, (t0, t1, t2))]
        tail_w = jnp.exp(t0 - col(0, b))
        tail_n = pair(jnp.exp(t1 - col(1, b)), jnp.exp(t2 - col(2, b)))
        state_w = jnp.exp(t0) * state_w + dot_rows((kwr * tail_w).astype(BF16), vw[rs, :])
        grown = dot_rows((knr * tail_n).astype(BF16), vn[rs, :])
        state_n = jnp.where(low_row, jnp.exp(t1), jnp.exp(t2)) * state_n + jnp.where(diagonal, grown, 0.0)
    small = lax.broadcasted_iota(jnp.int32, (16, 128), 0)
    rates = jnp.where(small == 0, jnp.exp(sums[0]), jnp.where(small == 1, jnp.exp(sums[1]), jnp.exp(sums[2])))
    st_buf[0, 0:128, :] = state_w.astype(BF16)
    st_buf[0, 128:192, :] = (state_n[0:HDN, :] + state_n[HDN:128, :]).astype(BF16)
    st_buf[0, 192:208, :] = rates.astype(BF16)
    state_y = send(st_buf.at[0], st_buf.at[1], y_dev)
    cross_up = [send(up_half(oy, 0), up_at(z, y, 0), y_dev)]

    for b in range(NB):
        rs = pl.ds(b * BLOCK, BLOCK)
        kwr, knr = k_rot[rs, 0:128], k_rot[rs, 128:256]
        qwr = turned(qw[rs, :].astype(F32), tables(0, b), 0)
        qnr = turned(qn[rs, :].astype(F32), tables(1, b), 1)

        def factor(h):
            return jnp.where(lower, jnp.exp(jnp.minimum(col(h, b) - line(h, b), 0.0)), 0.0)

        scores = (dot_cols(qwr.astype(BF16), kwr) * factor(0)).astype(BF16)
        inside[rs, 0:128] = dot(scores, vw[rs, :])
        near = (dot_cols(jnp.where(low, qnr, 0.0).astype(BF16), knr) * factor(1)).astype(BF16)
        far = (dot_cols(jnp.where(low, 0.0, qnr).astype(BF16), knr) * factor(2)).astype(BF16)
        inside[rs, 128:256] = pair(dot(near, vn[rs, :]), dot(far, vn[rs, :]))
        k_rot[rs, 0:128] = (qwr * jnp.exp(col(0, b))).astype(BF16)
        k_rot[rs, 128:256] = (qnr * pair(jnp.exp(col(1, b)), jnp.exp(col(2, b)))).astype(BF16)

    def state(i):
        return st_buf[i, 0:128, :].astype(F32), st_buf[i, 128:192, :].astype(F32), st_buf[i, 192:208, :].astype(F32)

    def chained(first, second):
        r = second[2]
        return (
            first[0] * r[0:1, :] + second[0],
            first[1] * jnp.where(low_half, r[1:2, :], r[2:3, :]) + second[1],
            first[2] * r,
        )

    state_y.wait_recv()
    mine, theirs = state(0), state(1)
    lead = [jnp.where(y == 0, a, b) for a, b in zip(mine, theirs)]
    rear = [jnp.where(y == 0, b, a) for a, b in zip(mine, theirs)]
    plane = chained(lead, rear)
    st_buf[2, 0:128, :] = plane[0].astype(BF16)
    st_buf[2, 128:192, :] = plane[1].astype(BF16)
    st_buf[2, 192:208, :] = plane[2].astype(BF16)

    def state_copy(k, zs, zz):
        return pltpu.make_async_remote_copy(
            src_ref=st_buf.at[2], dst_ref=st_buf.at[3 + zs], send_sem=ssem.at[k], recv_sem=srecv.at[zs],
            device_id=dev(zz), device_id_type=MESH_ID,
        )

    state_sends = []
    for d in range(NZ - 1, 0, -1):
        copy = state_copy(link(), z, (z + d) % NZ)
        state_sends.append((z + d < NZ, copy))

        @pl.when(z + d < NZ)
        def _(copy=copy):
            copy.start()

    up_send(z, y, 1, up_half(y, 1), goal_z, z_copies)
    for copy in ow_first:
        copy.wait_recv()
    ow_y = send(ow_buf.at[side, :, relay_cols(y)], ow_buf.at[side, :, relay_cols(y)], y_dev)
    cross_up.append(send(up_half(oy, 1), up_at(z, y, 1), y_dev))
    ow_hand = [send(ow_buf.at[side, :, relay_cols(y)], ow_buf.at[side, :, relay_cols(y)], mate_dev)]

    for zs in range(NZ - 1):
        @pl.when(zs < z)
        def _(zs=zs):
            state_copy(0, zs, mz).wait_recv()

    held = (jnp.zeros((128, 128), F32), jnp.zeros((HDN, 128), F32), jnp.zeros((16, 128), F32))
    for zs in range(NZ - 1):
        held = [jnp.where(zs < z, a, b) for a, b in zip(chained(held, state(3 + zs)), held)]
    held = [jnp.where(y == 1, a, b) for a, b in zip(chained(held, theirs), held)]
    s_w = held[0]
    s_n = jnp.concatenate([jnp.where(low_half, held[1], 0.0), jnp.where(low_half, 0.0, held[1])], axis=0)

    sums = [jnp.zeros((1, 1), F32) for _ in range(3)]
    for b in range(NB):
        rs = pl.ds(b * BLOCK, BLOCK)
        whole_w = before[0, b] + jnp.exp(sums[0]) * s_w
        whole_n = before[1, b] + jnp.where(low_row, jnp.exp(sums[1]), jnp.exp(sums[2])) * s_n
        sums = [s + total(h, b) for h, s in enumerate(sums)]
        o_w = inside[rs, 0:128] + dot(k_rot[rs, 0:128], whole_w.astype(BF16))
        o_n = inside[rs, 128:256] + dot(k_rot[rs, 128:256], whole_n.astype(BF16))

        def both(v):
            first = jnp.sum(jnp.where(low, v, 0.0), axis=-1, keepdims=True) / HDN
            second = jnp.sum(jnp.where(low, 0.0, v), axis=-1, keepdims=True) / HDN
            return pair(first, second)

        c_w = o_w - jnp.mean(o_w, axis=-1, keepdims=True)
        n_w = c_w * lax.rsqrt(jnp.mean(c_w * c_w, axis=-1, keepdims=True) + head_eps)
        c_n = o_n - both(o_n)
        n_n = c_n * lax.rsqrt(both(c_n * c_n) + head_eps)
        mixed[rs, 0:128] = (jax.nn.silu(gw[rs, :].astype(F32)) * n_w).astype(BF16)
        mixed[rs, 128:256] = (jax.nn.silu(gn[rs, :].astype(F32)) * n_n).astype(BF16)

    def my_rows(i):
        return pl.ds(pl.multiple_of(i * RT, RT), RT)

    swaps = [
        send(mixed.at[my_rows((x + dx) % 2 * 2 + (c + dc) % 2), :], mix_in.at[tp], dev(z, 0, dx, dc))
        for dx, dc in ((1, 0), (1, 1), (0, 1))
    ]
    cross_down = [
        send(down_half(oy, 0), down_buf.at[sp, pl.ds(0, HF), :], y_dev)
    ]
    mix_in[tp] = mixed[my_rows(tp), :]
    cross_up[0].wait_recv()
    up_send(z, oy, 0, up_at(z, oy, 0), goal_z, z_copies)
    for copy in ow_main:
        copy.wait_recv()
    ow_hand.append(send(ow_buf.at[side, :, main_cols], ow_buf.at[side, :, main_cols], mate_dev))
    ow_y.wait_recv()
    ow_hand.append(send(ow_buf.at[side, :, relay_cols(oy)], ow_buf.at[side, :, relay_cols(oy)], mate_dev))
    for copy in ow_mate + ow_hand + swaps:
        copy.wait_recv()
    for copy in locals_:
        copy.wait()

    def project(i, _):
        cs = pl.ds(pl.multiple_of(i * 512, 512), 512)
        acc = stream[:, cs].astype(F32)
        for j in range(TP):
            acc = acc + dot(mix_in[j], ow_buf[j, :, cs])
        mid[:, cs] = acc.astype(BF16)
        return 0

    lax.fori_loop(0, D // 512, project, 0)

    own_set = jnp.where(heavy, 0, 1)

    def unit(s, dy, dx, h, dc=0):
        return (((s * 2 + (y + dy) % 2) * 2 + (x + dx) % 2) * 2 + h) * 2 + (c + dc) % 2

    NS = 32

    def norm(i, _):
        m = mid[pl.ds(pl.multiple_of(i * NS, NS), NS), :].astype(F32)
        scale = lax.rsqrt(jnp.mean(m * m, axis=-1, keepdims=True) + norm_eps)
        per = RH // NS
        rows[unit(own_set, 0, 0, i // per), pl.ds(pl.multiple_of(i % per * NS, NS), NS), :] = (
            m * scale * gain[...].astype(F32)
        ).astype(BF16)
        return 0

    lax.fori_loop(0, RT // NS, norm, 0)

    def piece(s, dy, dx, h):
        return rows.at[unit(s, dy, dx, h)]

    def pass_on(s, dy, dx, h, device):
        return send(piece(s, dy, dx, h), piece(s, dy, dx, h), device)

    z_units = [(link(), u) for u in ((0, 0, 0), (0, 0, 1), (0, 1, 0), (1, 0, 1))]
    z_parts = [(link(), link()) for _ in range(SP)]
    common = list(pending)
    pending.clear()

    def cols_of(j):
        return pl.ds(pl.multiple_of(j * CB, CB), CB)

    def put(j, h, a, b):
        rs = pl.ds(h * RH, RH)
        out[rs, cols_of(j)] = (mid[rs, cols_of(j)].astype(F32) + a.astype(F32) + b.astype(F32)).astype(BF16)

    @pl.when(is_end)
    def _():
        sent = []

        def z_unit(i):
            k, (dy, dx, h) = z_units[i]
            start(k, piece(1, dy, dx, h), piece(1, dy, dx, h), dev(pz))

        side_x = pass_on(1, 0, 0, 0, x_dev)
        side_y = pass_on(1, 0, 0, 1, y_dev)
        cross_up[1].wait_recv()
        up_send(z, oy, 1, up_at(z, oy, 1), goal_z, sent)
        z_unit(0)
        z_unit(1)
        cross_down.append(
            send(down_half(oy, 1), down_buf.at[sp, pl.ds(HF, HF), :], y_dev)
        )
        side_x.wait_recv()
        z_unit(2)
        side_y.wait_recv()
        z_unit(3)
        for copy in cross_down:
            copy.wait_recv()
        for yy in range(2):
            down_send(z, yy, down_at(z, yy), goal_z, sent)
        order = [(zs, yy) for zs in (pz, NZ - 1 - pz, z, NZ - 1 - z) for yy in range(2)]
        done = []
        for k, (zs, yy) in enumerate(order):
            ka, kb = z_parts[k]
            arrive(ka, z_in.at[k, 0])
            a = send(z_in.at[k, 0, oy], last_in.at[k, 0], y_dev)
            arrive(kb, z_in.at[k, 1])
            b = send(z_in.at[k, 1, ox], last_in.at[k, 1], x_dev)
            done.append((k, zs * 2 + yy, a, b))
            if k:
                end_finish(done[k - 1], z_in, last_in, put, x, y)
        end_finish(done[-1], z_in, last_in, put, x, y)
        for copy in sent + pending:
            copy.wait_send()
        pending.clear()
        cross_down.pop()

    @pl.when(heavy)
    def _():
        sent = []
        hands = {}

        def hand(s, dy, dx, h):
            hands[s, dy, dx, h] = pass_on(s, dy, dx, h, mate_dev)

        def z_arrive(i):
            k, (dy, dx, h) = z_units[i]
            arrive(k, piece(1, dy, dx, h))
            return pass_on(1, dy, dx, h, x_dev if h else y_dev)

        def up_relay(yy):
            for i in range(2):
                up_wait(pz, yy, i)
                up_send(pz, yy, i, up_at(pz, yy, i), mz, sent)

        xa = pass_on(0, 0, 0, 0, x_dev)
        yb = pass_on(0, 0, 0, 1, y_dev)
        xb = pass_on(0, 0, 0, 1, x_dev)
        ya = pass_on(0, 0, 0, 0, y_dev)
        hand(0, 0, 0, 0)
        hand(0, 0, 0, 1)
        cross_down.append(
            send(down_half(oy, 1), down_buf.at[sp, pl.ds(HF, HF), :], y_dev)
        )
        up_relay(y)
        cross_up[1].wait_recv()
        up_send(z, oy, 1, up_at(z, oy, 1), goal_z, sent)
        xa.wait_recv()
        corner_a = pass_on(0, 0, 1, 0, y_dev)
        hand(0, 0, 1, 0)
        yb.wait_recv()
        corner_b = pass_on(0, 1, 0, 1, x_dev)
        hand(0, 1, 0, 1)
        up_relay(oy)
        down_send(z, y, down_at(z, y), goal_z, sent)
        ends = {}
        ends[1, 0, 0] = z_arrive(0)
        hand(1, 0, 0, 0)
        xb.wait_recv()
        hand(0, 0, 1, 1)
        ya.wait_recv()
        hand(0, 1, 0, 0)
        ends[0, 1, 1] = z_arrive(1)
        hand(1, 0, 0, 1)
        for copy in cross_down:
            copy.wait_recv()
        down_send(z, oy, down_at(z, oy), goal_z, sent)
        corner_a.wait_recv()
        hand(0, 1, 1, 0)
        corner_b.wait_recv()
        hand(0, 1, 1, 1)
        for zs in (mz, NZ - 1 - pz):
            for yy in range(2):
                for i in range(2):
                    up_wait(zs, yy, i)

        def up_rows(s, dy, dx):
            for h in range(2):
                hands[s, dy, dx, h].wait_recv()
            i = (s * 2 + (y + dy) % 2) * 2 + (x + dx) % 2
            us = pl.ds(pl.multiple_of(i * 4, 4), 4)

            def one(j, _):
                cs = pl.ds(pl.multiple_of(j * 512, 512), 512)
                h = jnp.maximum(dot(rows[us].reshape(2 * RT, D), up_buf[:, cs]), 0.0)
                hidden[i, :, cs] = (h * h).astype(BF16)
                return 0

            lax.fori_loop(0, FH // 512, one, 0)

        up_rows(0, 0, 0)
        ends[1, 1, 0] = z_arrive(2)
        hand(1, 0, 1, 0)
        up_rows(0, 0, 1)
        ends[1, 1, 1] = z_arrive(3)
        hand(1, 1, 0, 1)
        up_rows(0, 1, 0)
        up_rows(0, 1, 1)

        chain = (z, mz, pz, NZ - 1 - pz)
        chunks = (
            [(0, 0, yy) for yy in range(2)] + [(0, 1, yy) for yy in range(2)]
            + [(1, 0, yy) for yy in range(2)] + [(1, 1, yy) for yy in range(2)]
            + [(s, i, yy) for i in (2, 3) for yy in range(2) for s in range(2)]
        )
        waited = set()
        relays = []
        slots = part.shape[0]
        stage = [dict() for _ in chunks]
        of_set = [sum(1 for t in chunks[:k] if t[0] == chunks[k][0]) for k in range(len(chunks))]

        def down_ready(i, yy):
            if (i, yy) in waited or i == 0:
                return
            waited.add((i, yy))
            down_wait(chain[i], yy)
            if i == 2:
                down_send(pz, yy, down_at(pz, yy), mz, sent)

        def multiply(k):
            s, i, yy = chunks[k]
            down_ready(i, yy)
            if k >= slots:
                for copy in stage[k - slots]["sent"]:
                    copy.wait_send()
            j = chain[i] * 2 + yy
            slot = k % slots

            def one(q, _):
                got = dot(hidden[s * 4 + q], down_buf[j]).astype(BF16)
                part[slot, q // 2, q % 2] = got.reshape(2, 2, RH, CB)
                return 0

            lax.fori_loop(0, 4, one, 0)
            mate = copy_of(link(), part.at[slot, :, :, :, 1 - c], mate_in.at[k], mate_dev)
            mate.start()
            stage[k]["mate"] = mate
            stage[k]["sent"] = [mate]

        def fold(k):
            slot = k % slots
            stage[k]["mate"].wait_recv()

            def one(q, _):
                for h in range(2):
                    part[slot, q // 2, q % 2, h, c] = (
                        part[slot, q // 2, q % 2, h, c].astype(F32) + mate_in[k, q // 2, q % 2, h].astype(F32)
                    ).astype(BF16)
                return 0

            lax.fori_loop(0, 4, one, 0)
            to_x = copy_of(link(), part.at[slot, :, ox, 0, c], x_in.at[k], x_dev)
            to_x.start()
            to_y = copy_of(link(), part.at[slot, oy, :, 1, c], y_in.at[k], y_dev)
            to_y.start()
            stage[k]["x"], stage[k]["y"] = to_x, to_y
            stage[k]["sent"] += [to_x, to_y]

        def spread(k):
            slot = k % slots
            s = chunks[k][0]
            stage[k]["x"].wait_recv()
            for i in range(2):
                part[slot, i, x, 0, c] = (
                    part[slot, i, x, 0, c].astype(F32) + x_in[k, i].astype(F32)
                ).astype(BF16)
            n = of_set[k]
            if s:
                a = copy_of(z_parts[n][0], part.at[slot, :, x, 0, c], z_in.at[n, 0], dev(pz))
            else:
                a = copy_of(link(), part.at[slot, oy, x, 0, c], last_in.at[n, 0], y_dev)
            a.start()
            stage[k]["y"].wait_recv()
            for i in range(2):
                part[slot, y, i, 1, c] = (
                    part[slot, y, i, 1, c].astype(F32) + y_in[k, i].astype(F32)
                ).astype(BF16)
            if s:
                b = copy_of(z_parts[n][1], part.at[slot, y, :, 1, c], z_in.at[n, 1], dev(pz))
            else:
                b = copy_of(link(), part.at[slot, y, ox, 1, c], last_in.at[n, 1], x_dev)
            b.start()
            stage[k]["last"] = (a, b)
            stage[k]["sent"] += [a, b]

        def finish(k):
            s, i, yy = chunks[k]
            if s:
                return
            slot = k % slots
            n = of_set[k]
            j = chain[i] * 2 + yy
            for h, copy in enumerate(stage[k]["last"]):
                copy.wait_recv()
                put(j, h, part[slot, y, x, h, c], last_in[n, h])

        reached = [0, 0, 0]

        def advance(which, limit):
            for k in range(reached[which], max(limit, reached[which])):
                (fold, spread, finish)[which](k)
            reached[which] = max(limit, reached[which])

        n_chunks = len(chunks)
        for k in range(n_chunks):
            if k == 4:
                advance(0, k)
                ends[1, 0, 0].wait_recv()
                hand(1, 1, 0, 0)
                ends[0, 1, 1].wait_recv()
                hand(1, 0, 1, 1)
                up_rows(1, 0, 0)
                advance(1, 1)
                up_rows(1, 0, 1)
                advance(1, 2)
                ends[1, 1, 0].wait_recv()
                hand(1, 1, 1, 0)
                ends[1, 1, 1].wait_recv()
                hand(1, 1, 1, 1)
                up_rows(1, 1, 0)
                advance(1, 3)
                up_rows(1, 1, 1)
                down_ready(2, 0)
            elif k in (10, 12, 14):
                advance(0, k)
                advance(1, k - 1)
                advance(2, k - 3)
            else:
                advance(2, k - 6)
                advance(1, k - 4)
                advance(0, k - 2)
            if k == 7:
                down_ready(2, 1)
            multiply(k)
        for k in range(n_chunks - 2, n_chunks + 1):
            advance(0, k)
            advance(1, k - 1)
            advance(2, k - 3)
        advance(1, n_chunks)
        advance(2, n_chunks)
        for k in range(n_chunks - slots, n_chunks):
            for copy in stage[k]["sent"]:
                copy.wait_send()
        for copy in sent + pending:
            copy.wait_send()
        pending.clear()

    for when, copy in state_sends:
        @pl.when(when)
        def _(copy=copy):
            copy.wait_send()
    for copy in common + z_copies:
        copy.wait_send()


def end_finish(one, z_in, last_in, put, x, y):
    k, j, a, b = one
    a.wait_recv()
    put(j, 0, z_in[k, 0, y], last_in[k, 0])
    b.wait_recv()
    put(j, 1, z_in[k, 1, x], last_in[k, 1])


def one_kernel(SP, TP, *args):
    (stream, qw, kw, vw, gw, dw, qn, kn, vn, gn, dn, ow, on, gain, up, down) = args
    T = qw.shape[0]
    NB = T // BLOCK
    D = stream.shape[1]
    RT = T // TP
    RH = RT // 2
    FH = up.shape[1] // 2
    CB = down.shape[1]
    heads = dw.shape[0] + dn.shape[0]
    decay = jnp.concatenate([dw, dn]).reshape(heads * NB, BLOCK)
    decay = jnp.pad(decay, ((0, 128 - heads * NB), (0, 0)))
    offs, starts = turn_tables(SP, T)
    vmem = pl.BlockSpec(memory_space=pltpu.VMEM)
    hbm = pl.BlockSpec(memory_space=pl.ANY)
    copies = 256
    return pl.pallas_call(
        functools.partial(layer_kernel, SP, TP),
        out_shape=jax.ShapeDtypeStruct((RT, D), BF16),
        in_specs=[vmem] * 13 + [hbm] * 4,
        out_specs=vmem,
        scratch_shapes=[
            pltpu.VMEM((D, FH), BF16),
            pltpu.VMEM((SP, FH, CB), BF16),
            pltpu.VMEM((TP, 256, D), BF16),
            pltpu.VMEM((7, 208, 128), BF16),
            pltpu.VMEM((T, 256), BF16),
            pltpu.VMEM((2, NB, 128, 128), F32),
            pltpu.VMEM((T, 256), F32),
            pltpu.VMEM((T, 256), BF16),
            pltpu.VMEM((TP, RT, 256), BF16),
            pltpu.VMEM((RT, D), BF16),
            pltpu.VMEM((32, RH, D), BF16),
            pltpu.VMEM((8, 2 * RT, FH), BF16),
            pltpu.VMEM((8, 2, 2, 2, 2, RH, CB), BF16),
            pltpu.VMEM((2 * SP, 2, 2, 2, RH, CB), BF16),
            pltpu.VMEM((2 * SP, 2, RH, CB), BF16),
            pltpu.VMEM((2 * SP, 2, RH, CB), BF16),
            pltpu.VMEM((SP, 2, RH, CB), BF16),
            pltpu.VMEM((SP, 2, 2, RH, CB), BF16),
            pltpu.SemaphoreType.DMA((copies,)),
            pltpu.SemaphoreType.DMA((copies,)),
            pltpu.SemaphoreType.DMA((8,)),
            pltpu.SemaphoreType.DMA((24,)),
            pltpu.SemaphoreType.DMA((24,)),
            pltpu.SemaphoreType.DMA((4,)),
        ],
        compiler_params=pltpu.CompilerParams(
            collective_id=0, has_side_effects=True, vmem_limit_bytes=63 * 1024 * 1024
        ),
    )(stream, qw, kw, vw, gw, qn, kn, vn, gn, decay, jnp.asarray(offs), jnp.asarray(starts),
      gain.reshape(1, D), ow, on, up, down)


def fits_kernel(SP, TP, args):
    D, FF = args[14].shape
    T = args[1].shape[0] // SP
    return (
        SP == 8 and TP == 4 and D % (SP * 128) == 0 and T % (TP * 32) == 0 and T % BLOCK == 0
        and args[1].shape[1] == TP * 128 and args[6].shape[1] == TP * 128
    )


def solution(mesh):
    in_specs = (
        P(("sp", "tp"), None),
        P("sp", "tp"),
        P("sp", "tp"),
        P("sp", "tp"),
        P("sp", "tp"),
        P("tp", "sp"),
        P("sp", "tp"),
        P("sp", "tp"),
        P("sp", "tp"),
        P("sp", "tp"),
        P("tp", "sp"),
        P("tp", None),
        P("tp", None),
        P(),
        P("sp", "tp"),
        P("tp", "sp"),
    )
    out_specs = P(("sp", "tp"), None)
    SP, TP = mesh.shape["sp"], mesh.shape["tp"]

    def layer(*args):
        body = functools.partial(one_kernel, SP, TP) if fits_kernel(SP, TP, args) else on_device
        return jax.shard_map(
            body, mesh=mesh, in_specs=in_specs, out_specs=out_specs, check_vma=False
        )(*args)

    return layer
```

```python
import functools
import jax
import jax.numpy as jnp
import numpy as np
from jax import lax
from jax.experimental import pallas as pl
from jax.experimental.pallas import tpu as pltpu
from jax.sharding import PartitionSpec as P

HDW = 128
HDN = 64
BLOCK = 128


head_eps = 1e-05
norm_eps = 1e-06
rope_base = 10000.0


def carried_in(shard, axis, join, neutral):
    place = lax.axis_index(axis)
    gathered = jax.tree.map(
        lambda a, kind: lax.all_gather(a.astype(kind), axis),
        shard,
        (jnp.bfloat16, jnp.bfloat16, jnp.bfloat16, jnp.bfloat16),
    )
    state = jax.tree.map(lambda a, e: jnp.zeros_like(a) + jnp.asarray(e, a.dtype), shard, neutral)

    def one(turn, state):
        return join(
            state,
            jax.tree.map(
                lambda a, own: lax.dynamic_index_in_dim(a, turn, 0, False).astype(own.dtype),
                gathered,
                shard,
            ),
        )

    return lax.fori_loop(0, place, one, state)


def rotate(values, places):
    half = values.shape[-1] // 2
    inverse = rope_base ** (-jnp.arange(half, dtype=jnp.float32) / half)
    angles = places[:, None] * inverse[None, :]
    cosine = jnp.cos(angles)[:, None, :]
    sine = jnp.sin(angles)[:, None, :]
    front = values[..., :half]
    back = values[..., half:]
    return jnp.concatenate([front * cosine - back * sine, back * cosine + front * sine], axis=-1)


def block_step(carried, inputs):
    query, keys, values, log_rate = inputs
    running = jnp.cumsum(log_rate, axis=0)
    spread = running[:, None, :] - running[None, :, :]
    length = log_rate.shape[0]
    lower = (jnp.arange(length)[:, None] >= jnp.arange(length)[None, :])[:, :, None]
    factor = jnp.where(lower, jnp.exp(jnp.minimum(spread, 0.0)), 0.0)
    scores = jnp.einsum("thd,shd->tsh", query, keys) * factor
    within = jnp.einsum("tsh,she->the", scores, values)
    across = jnp.einsum("thd,hde->the", query, carried) * jnp.exp(running)[:, :, None]
    tail_decay = jnp.exp(running[-1][None, :] - running)
    updated = jnp.exp(running[-1])[:, None, None] * carried + jnp.einsum(
        "shd,she->hde", keys * tail_decay[:, :, None], values
    )
    return (updated, within + across)


def head_norm(values):
    centre = values - jnp.mean(values, axis=-1, keepdims=True)
    spread = jnp.mean(centre * centre, axis=-1, keepdims=True)
    return centre * lax.rsqrt(spread + head_eps)


def local_group(query, keys, values, log_rate, width, places):
    length = query.shape[0]
    count_of_heads = query.shape[1] // width
    blocks = length // BLOCK

    def split(array):
        return array.astype(jnp.float32).reshape(length, count_of_heads, width)

    query_rot = rotate(split(query), places)
    keys_rot = rotate(split(keys), places) * width ** (-0.5)
    rates = log_rate.T
    carried = jnp.zeros((count_of_heads, width, width), jnp.float32)
    final_state, outputs = lax.scan(
        block_step,
        carried,
        (
            query_rot.reshape(blocks, BLOCK, count_of_heads, width),
            keys_rot.reshape(blocks, BLOCK, count_of_heads, width),
            split(values).reshape(blocks, BLOCK, count_of_heads, width),
            rates.reshape(blocks, BLOCK, count_of_heads),
        ),
    )
    running = jnp.cumsum(rates, axis=0)
    return (
        query_rot,
        outputs.reshape(length, count_of_heads, width),
        final_state,
        jnp.exp(running[-1]),
        running,
    )


def finish_group(query_rot, outputs, incoming, running, gate):
    length = outputs.shape[0]
    outputs = (
        outputs + jnp.einsum("thd,hde->the", query_rot, incoming) * jnp.exp(running)[:, :, None]
    )
    normed = head_norm(outputs).reshape(length, -1)
    return (jax.nn.silu(gate.astype(jnp.float32)) * normed).astype(jnp.bfloat16)


def chain(earlier, later):
    rate_wide, memory_wide, rate_narrow, memory_narrow = earlier
    later_rate_wide, later_memory_wide, later_rate_narrow, later_memory_narrow = later
    return (
        rate_wide * later_rate_wide,
        memory_wide * later_rate_wide[:, None, None] + later_memory_wide,
        rate_narrow * later_rate_narrow,
        memory_narrow * later_rate_narrow[:, None, None] + later_memory_narrow,
    )


def row_norm(middle, norm_gain):
    middle_f = middle.astype(jnp.float32)
    scale = lax.rsqrt(jnp.mean(middle_f * middle_f, axis=-1, keepdims=True) + norm_eps)
    return (middle_f * scale * norm_gain.astype(jnp.float32)).astype(jnp.bfloat16)


def on_device(
    stream_in,
    query_wide,
    key_wide,
    value_wide,
    gate_wide,
    decay_wide,
    query_narrow,
    key_narrow,
    value_narrow,
    gate_narrow,
    decay_narrow,
    output_wide,
    output_narrow,
    norm_gain,
    up_weight,
    down_weight,
):
    length = query_wide.shape[0]
    places = (lax.axis_index("sp") * length + jnp.arange(length, dtype=jnp.int32)).astype(
        jnp.float32
    )
    wide_query, wide_out, wide_state, wide_total, wide_running = local_group(
        query_wide, key_wide, value_wide, decay_wide, HDW, places
    )
    narrow_query, narrow_out, narrow_state, narrow_total, narrow_running = local_group(
        query_narrow, key_narrow, value_narrow, decay_narrow, HDN, places
    )
    identity = (
        jnp.ones_like(wide_total),
        jnp.zeros_like(wide_state),
        jnp.ones_like(narrow_total),
        jnp.zeros_like(narrow_state),
    )
    incoming = carried_in(
        (wide_total, wide_state, narrow_total, narrow_state), "sp", chain, identity
    )
    mixed_wide = finish_group(wide_query, wide_out, incoming[1], wide_running, gate_wide)
    mixed_narrow = finish_group(narrow_query, narrow_out, incoming[3], narrow_running, gate_narrow)
    mixed_sum = lax.psum_scatter(
        (
            jnp.dot(mixed_wide, output_wide, preferred_element_type=jnp.float32)
            + jnp.dot(mixed_narrow, output_narrow, preferred_element_type=jnp.float32)
        ).astype(jnp.bfloat16),
        "tp",
        scatter_dimension=0,
        tiled=True,
    ).astype(jnp.float32)
    middle = (stream_in.astype(jnp.float32) + mixed_sum).astype(jnp.bfloat16)
    normed = lax.all_gather(row_norm(middle, norm_gain), "tp", axis=0, tiled=True)
    up_sum = jnp.dot(
        normed,
        lax.all_gather(up_weight, "sp", axis=0, tiled=True),
        preferred_element_type=jnp.float32,
    )
    hidden = jnp.square(jax.nn.relu(up_sum)).astype(jnp.bfloat16)
    down_sum = jnp.dot(
        hidden,
        lax.all_gather(down_weight, "sp", axis=1, tiled=True),
        preferred_element_type=jnp.float32,
    )
    down_rows = lax.psum_scatter(
        down_sum.astype(jnp.bfloat16), "tp", scatter_dimension=0, tiled=True
    ).astype(jnp.float32)
    return (middle.astype(jnp.float32) + down_rows).astype(jnp.bfloat16)


F32 = jnp.float32
BF16 = jnp.bfloat16
MESH_ID = pl.DeviceIdType.MESH


def turn_tables(shards, length):
    lane = np.arange(128)
    offsets, starts = [], []
    for width in (HDW, HDN):
        half = width // 2
        inverse = rope_base ** (-((lane % half).astype(np.float64)) / half)
        inside = np.arange(BLOCK)[:, None] * inverse[None, :]
        first = (np.arange(shards * length // BLOCK) * BLOCK)[:, None] * inverse[None, :]
        offsets += [np.cos(inside), np.sin(inside)]
        starts += [np.cos(first), np.sin(first)]
    return np.stack(offsets).astype(np.float32), np.stack(starts).astype(np.float32)


def dot(a, b):
    return jnp.dot(a, b, preferred_element_type=F32)


def dot_rows(a, b):
    return lax.dot_general(a, b, (((0,), (0,)), ((), ())), preferred_element_type=F32)


def dot_cols(a, b):
    return lax.dot_general(a, b, (((1,), (1,)), ((), ())), preferred_element_type=F32)


N_CHUNKS = 16
OWN_LEAD = 4
SLOTS = 8


def chunk_at(k):
    t = k - OWN_LEAD
    if isinstance(k, int):
        if t < 0:
            return 0, k // 2, k % 2
        far = t % 3 != 2 if t < 8 else t < 10
        n = (t - t // 3 if far else 4 + t // 3) if t < 8 else (t - 2 if far else t - 4)
        return int(far), n // 2, n % 2
    far = jnp.where(t < 8, jnp.where(t % 3 != 2, 1, 0), jnp.where(t < 10, 1, 0)) == 1
    early = jnp.where(far, t - t // 3, 4 + t // 3)
    n = jnp.where(t < 0, k, jnp.where(t < 8, early, jnp.where(far, t - 2, t - 4)))
    return jnp.where((t >= 0) & far, 1, 0), n // 2, n % 2


def chunk_kind(k):
    s, i, yy = chunk_at(k)
    n = i * 2 + yy
    last = (s == 1) & (yy == 1) & (i < 3)
    return s, n, last


def layer_kernel(
    SP, TP,
    stream, qw, kw, vw, gw, qn, kn, vn, gn, dw, dn, offs, starts, gain, ow_w, ow_n, up, down,
    out,
    up_buf, down_buf, ow_buf, st_buf, k_rot, before, inside, mixed, mix_in, mid, rows, hidden, part,
    mate_in, x_in, y_in, last_in, z_in, z_done, rates_buf, up_sum,
    ssem, rsem, lsem, zsend, zrecv, srecv,
):
    sp = lax.axis_index("sp")
    tp = lax.axis_index("tp")
    NZ = SP // 2
    z, y = sp // 2, sp % 2
    x, c = tp // 2, tp % 2
    T = qw.shape[0]
    NB = T // BLOCK
    RT = T // TP
    RH = RT // 2
    RB = up.shape[0]
    CB = down.shape[1]
    D = stream.shape[1]
    FH = up.shape[1] // 2
    heavy = (z == 1) | (z == 2)
    is_end = jnp.logical_not(heavy)
    pz = z + 1 - 2 * (z % 2)
    mz = NZ - 1 - z
    goal_z = jnp.where(heavy, mz, pz)

    def dev(zz, dy=0, dx=0, dc=0):
        return (zz * 2 + (y + dy) % 2, (x + dx) % 2 * 2 + (c + dc) % 2)

    x_dev, y_dev, mate_dev = dev(z, 0, 1), dev(z, 1), dev(z, 0, 0, 1)
    count = [0]
    pending = []

    def link():
        count[0] += 1
        return count[0] - 1

    def copy_of(k, src, dst, device):
        return pltpu.make_async_remote_copy(
            src_ref=src, dst_ref=dst, send_sem=ssem.at[k], recv_sem=rsem.at[k],
            device_id=device, device_id_type=MESH_ID,
        )

    def start(k, src, dst, device):
        copy = copy_of(k, src, dst, device)
        copy.start()
        pending.append(copy)
        return copy

    def send(src, dst, device):
        return start(link(), src, dst, device)

    def arrive(k, dst):
        copy_of(k, dst, dst, mate_dev).wait_recv()

    barrier = pltpu.get_barrier_semaphore()
    for d in range(1, NZ):
        pl.semaphore_signal(barrier, inc=1, device_id=dev((z + d) % NZ), device_id_type=MESH_ID)
    for device in (x_dev, y_dev, mate_dev, dev(z, 0, 1, 1)):
        pl.semaphore_signal(barrier, inc=1, device_id=device, device_id_type=MESH_ID)
    pl.semaphore_wait(barrier, NZ + 3)

    locals_ = []

    def keep(src, dst):
        copy = pltpu.make_async_copy(src, dst, lsem.at[len(locals_)])
        copy.start()
        locals_.append(copy)
        return copy

    HB = RB // 2
    HF = FH // 2

    def up_at(zs, yy, part_of):
        return up_buf.at[pl.ds(pl.multiple_of((zs * 2 + yy) * RB + part_of * HB, HB), HB), :]

    def down_at(zs, yy, part_of):
        return down_buf.at[zs * 2 + yy, pl.ds(part_of * HF, HF), :]

    def up_half(half, part_of):
        return up.at[pl.ds(part_of * HB, HB), pl.ds(pl.multiple_of(half * FH, FH), FH)]

    def down_half(half, part_of):
        return down.at[pl.ds(pl.multiple_of(half * FH + part_of * HF, HF), HF), :]

    z_copies = []

    def z_copy(slot, sem, src, dst, zz):
        return pltpu.make_async_remote_copy(
            src_ref=src, dst_ref=dst, send_sem=zsend.at[slot], recv_sem=zrecv.at[sem],
            device_id=dev(zz), device_id_type=MESH_ID,
        )

    def up_sem(zs, yy, part_of):
        return (zs * 2 + yy) * 2 + part_of

    def down_sem(zs, yy, part_of):
        return 4 * NZ + up_sem(zs, yy, part_of)

    z_slots = [0]

    def z_slot():
        z_slots[0] += 1
        return z_slots[0] - 1

    def up_send(zs, yy, part_of, src, zz, into):
        copy = z_copy(z_slot(), up_sem(zs, yy, part_of), src, up_at(zs, yy, part_of), zz)
        copy.start()
        into.append(copy)

    def down_send(zs, yy, part_of, zz, into):
        ref = down_at(zs, yy, part_of)
        copy = z_copy(z_slot(), down_sem(zs, yy, part_of), ref, ref, zz)
        copy.start()
        into.append(copy)

    def up_wait(zs, yy, part_of):
        ref = up_at(zs, yy, part_of)
        z_copy(0, up_sem(zs, yy, part_of), ref, ref, goal_z).wait_recv()

    def down_wait(zs, yy, part_of):
        ref = down_at(zs, yy, part_of)
        z_copy(0, down_sem(zs, yy, part_of), ref, ref, goal_z).wait_recv()

    oy = 1 - y
    ox = 1 - x
    RW = D * 3 // 8
    QB = HB // 4

    def ow_at(i, g, cols):
        return ow_buf.at[i, pl.ds(g * 128, 128), cols]

    def relay_cols(yy):
        return pl.ds(pl.multiple_of(yy * (D - RW), 128), RW)

    main_cols = pl.ds(RW, D - 2 * RW)
    every = pl.ds(0, D)
    side = ox * 2 + c
    ow_first = [
        send(r.at[:, relay_cols(y)], ow_at(tp, g, relay_cols(y)), x_dev) for g, r in enumerate((ow_w, ow_n))
    ]
    ow_main = [
        send(r.at[:, main_cols], ow_at(tp, g, main_cols), x_dev) for g, r in enumerate((ow_w, ow_n))
    ]
    ow_mate = [send(r, ow_at(tp, g, every), mate_dev) for g, r in enumerate((ow_w, ow_n))]
    up_send(z, y, 0, up_half(y, 0), goal_z, z_copies)
    keep(ow_w, ow_at(tp, 0, every))
    keep(ow_n, ow_at(tp, 1, every))
    keep(up_half(y, 0), up_at(z, y, 0))
    keep(up_half(y, 1), up_at(z, y, 1))
    for i in range(2):
        keep(down_half(y, i), down_at(z, y, i))

    def cross_rows(first, many):
        return send(
            up.at[pl.ds(first, many), pl.ds(pl.multiple_of(oy * FH, FH), FH)],
            up_buf.at[pl.ds(pl.multiple_of(sp * RB + first, QB), many), :], y_dev,
        )

    cross_first = [cross_rows(0, QB)]

    lane = lax.broadcasted_iota(jnp.int32, (128, 128), 1)
    row = lax.broadcasted_iota(jnp.int32, (128, 128), 0)
    lower = row >= lane
    low = lane < HDN
    low_row = row < HDN
    low_half = lax.broadcasted_iota(jnp.int32, (HDN, 128), 1) < HDN
    diagonal = low == low_row
    for h in range(3):
        for b in range(NB):
            ref = dw if h == 0 else dn
            at = 0 if h == 0 else h - 1
            rates_buf[h * NB + b:h * NB + b + 1, :] = ref[at:at + 1, b * BLOCK:(b + 1) * BLOCK]
    cr = rates_buf[...]
    step = 1
    while step < 128:
        cr = cr + jnp.where(lane >= step, pltpu.roll(cr, step, 1), 0.0)
        step *= 2
    ct = cr.T

    def col(h, b):
        return ct[:, h * NB + b:h * NB + b + 1]

    def line(h, b):
        return cr[h * NB + b:h * NB + b + 1, :]

    def total(h, b):
        return cr[h * NB + b:h * NB + b + 1, 127:128]

    def pair(a, b):
        return jnp.where(low, a, b)

    sign_w = jnp.where(low, -1.0, 1.0)
    early = (lane % HDN) < HDN // 2
    sign_n = jnp.where(early, -1.0, 1.0)

    def tables(g, b):
        cb = starts[2 * g, pl.ds(sp * NB + b, 1), :]
        sb = starts[2 * g + 1, pl.ds(sp * NB + b, 1), :]
        co, so = offs[2 * g], offs[2 * g + 1]
        return co * cb - so * sb, (so * cb + co * sb) * (sign_n if g else sign_w)

    def turned(v, table, g):
        if g:
            other = jnp.where(early, pltpu.roll(v, 128 - HDN // 2, 1), pltpu.roll(v, HDN // 2, 1))
        else:
            other = pltpu.roll(v, HDW // 2, 1)
        return v * table[0] + other * table[1]

    state_w = jnp.zeros((128, 128), F32)
    state_n = jnp.zeros((128, 128), F32)
    sums = [jnp.zeros((1, 1), F32) for _ in range(3)]
    for b in range(NB):
        rs = pl.ds(b * BLOCK, BLOCK)
        before[0, b] = state_w
        before[1, b] = state_n
        kwr = turned(kw[rs, :].astype(F32), tables(0, b), 0) * HDW ** (-0.5)
        knr = turned(kn[rs, :].astype(F32), tables(1, b), 1) * HDN ** (-0.5)
        k_rot[rs, 0:128] = kwr.astype(BF16)
        k_rot[rs, 128:256] = knr.astype(BF16)
        t0, t1, t2 = total(0, b), total(1, b), total(2, b)
        sums = [s + t for s, t in zip(sums, (t0, t1, t2))]
        tail_w = jnp.exp(t0 - col(0, b))
        tail_n = pair(jnp.exp(t1 - col(1, b)), jnp.exp(t2 - col(2, b)))
        state_w = jnp.exp(t0) * state_w + dot_rows((kwr * tail_w).astype(BF16), vw[rs, :])
        grown = dot_rows((knr * tail_n).astype(BF16), vn[rs, :])
        state_n = jnp.where(low_row, jnp.exp(t1), jnp.exp(t2)) * state_n + jnp.where(diagonal, grown, 0.0)
    small = lax.broadcasted_iota(jnp.int32, (16, 128), 0)
    rates = jnp.where(small == 0, jnp.exp(sums[0]), jnp.where(small == 1, jnp.exp(sums[1]), jnp.exp(sums[2])))
    st_buf[0, 0:128, :] = state_w.astype(BF16)
    st_buf[0, 128:192, :] = (state_n[0:HDN, :] + state_n[HDN:128, :]).astype(BF16)
    st_buf[0, 192:208, :] = rates.astype(BF16)
    state_y = send(st_buf.at[0], st_buf.at[1], y_dev)
    cross_first.append(cross_rows(QB, HB - QB))

    for b in range(NB):
        rs = pl.ds(b * BLOCK, BLOCK)
        kwr, knr = k_rot[rs, 0:128], k_rot[rs, 128:256]
        qwr = turned(qw[rs, :].astype(F32), tables(0, b), 0)
        qnr = turned(qn[rs, :].astype(F32), tables(1, b), 1)

        def factor(h):
            return jnp.where(lower, jnp.exp(jnp.minimum(col(h, b) - line(h, b), 0.0)), 0.0)

        scores = (dot_cols(qwr.astype(BF16), kwr) * factor(0)).astype(BF16)
        inside[rs, 0:128] = dot(scores, vw[rs, :])
        near = (dot_cols(jnp.where(low, qnr, 0.0).astype(BF16), knr) * factor(1)).astype(BF16)
        far = (dot_cols(jnp.where(low, 0.0, qnr).astype(BF16), knr) * factor(2)).astype(BF16)
        inside[rs, 128:256] = pair(dot(near, vn[rs, :]), dot(far, vn[rs, :]))
        k_rot[rs, 0:128] = (qwr * jnp.exp(col(0, b))).astype(BF16)
        k_rot[rs, 128:256] = (qnr * pair(jnp.exp(col(1, b)), jnp.exp(col(2, b)))).astype(BF16)

    def state(i):
        return st_buf[i, 0:128, :].astype(F32), st_buf[i, 128:192, :].astype(F32), st_buf[i, 192:208, :].astype(F32)

    def chained(first, second):
        r = second[2]
        return (
            first[0] * r[0:1, :] + second[0],
            first[1] * jnp.where(low_half, r[1:2, :], r[2:3, :]) + second[1],
            first[2] * r,
        )

    state_y.wait_recv()
    mine, theirs = state(0), state(1)
    lead = [jnp.where(y == 0, a, b) for a, b in zip(mine, theirs)]
    rear = [jnp.where(y == 0, b, a) for a, b in zip(mine, theirs)]
    plane = chained(lead, rear)
    st_buf[2, 0:128, :] = plane[0].astype(BF16)
    st_buf[2, 128:192, :] = plane[1].astype(BF16)
    st_buf[2, 192:208, :] = plane[2].astype(BF16)

    def state_copy(k, zs, zz):
        return pltpu.make_async_remote_copy(
            src_ref=st_buf.at[2], dst_ref=st_buf.at[3 + zs], send_sem=ssem.at[k], recv_sem=srecv.at[zs],
            device_id=dev(zz), device_id_type=MESH_ID,
        )

    state_sends = []
    for d in range(NZ - 1, 0, -1):
        copy = state_copy(link(), z, (z + d) % NZ)
        state_sends.append((z + d < NZ, copy))

        @pl.when(z + d < NZ)
        def _(copy=copy):
            copy.start()

    up_send(z, y, 1, up_half(y, 1), goal_z, z_copies)
    ow_y = []
    for g, copy in enumerate(ow_first):
        copy.wait_recv()
        ow_y.append(send(ow_at(side, g, relay_cols(y)), ow_at(side, g, relay_cols(y)), y_dev))
    cross_last = send(up_half(oy, 1), up_at(z, y, 1), y_dev)
    ow_hand = [send(ow_buf.at[side, :, relay_cols(y)], ow_buf.at[side, :, relay_cols(y)], mate_dev)]

    for copy in cross_first:
        copy.wait_recv()
    up_send(z, oy, 0, up_at(z, oy, 0), goal_z, z_copies)
    for zs in range(NZ - 1):
        @pl.when(zs < z)
        def _(zs=zs):
            state_copy(0, zs, mz).wait_recv()

    held = (jnp.zeros((128, 128), F32), jnp.zeros((HDN, 128), F32), jnp.zeros((16, 128), F32))
    for zs in range(NZ - 1):
        held = [jnp.where(zs < z, a, b) for a, b in zip(chained(held, state(3 + zs)), held)]
    held = [jnp.where(y == 1, a, b) for a, b in zip(chained(held, theirs), held)]
    s_w = held[0]
    s_n = jnp.concatenate([jnp.where(low_half, held[1], 0.0), jnp.where(low_half, 0.0, held[1])], axis=0)

    sums = [jnp.zeros((1, 1), F32) for _ in range(3)]
    for b in range(NB):
        rs = pl.ds(b * BLOCK, BLOCK)
        whole_w = before[0, b] + jnp.exp(sums[0]) * s_w
        whole_n = before[1, b] + jnp.where(low_row, jnp.exp(sums[1]), jnp.exp(sums[2])) * s_n
        sums = [s + total(h, b) for h, s in enumerate(sums)]
        o_w = inside[rs, 0:128] + dot(k_rot[rs, 0:128], whole_w.astype(BF16))
        o_n = inside[rs, 128:256] + dot(k_rot[rs, 128:256], whole_n.astype(BF16))

        def both(v):
            first = jnp.sum(jnp.where(low, v, 0.0), axis=-1, keepdims=True) / HDN
            second = jnp.sum(jnp.where(low, 0.0, v), axis=-1, keepdims=True) / HDN
            return pair(first, second)

        c_w = o_w - jnp.mean(o_w, axis=-1, keepdims=True)
        n_w = c_w * lax.rsqrt(jnp.mean(c_w * c_w, axis=-1, keepdims=True) + head_eps)
        c_n = o_n - both(o_n)
        n_n = c_n * lax.rsqrt(both(c_n * c_n) + head_eps)
        mixed[rs, 0:128] = (jax.nn.silu(gw[rs, :].astype(F32)) * n_w).astype(BF16)
        mixed[rs, 128:256] = (jax.nn.silu(gn[rs, :].astype(F32)) * n_n).astype(BF16)

    def my_rows(i):
        return pl.ds(pl.multiple_of(i * RT, RT), RT)

    swaps = [
        send(mixed.at[my_rows((x + dx) % 2 * 2 + (c + dc) % 2), :], mix_in.at[tp], dev(z, 0, dx, dc))
        for dx, dc in ((1, 0), (1, 1), (0, 1))
    ]
    mix_in[tp] = mixed[my_rows(tp), :]
    for copy in ow_main:
        copy.wait_recv()
    ow_hand.append(send(ow_buf.at[side, :, main_cols], ow_buf.at[side, :, main_cols], mate_dev))
    for copy in ow_y:
        copy.wait_recv()
    ow_hand.append(send(ow_buf.at[side, :, relay_cols(oy)], ow_buf.at[side, :, relay_cols(oy)], mate_dev))
    for copy in ow_mate + ow_hand + swaps:
        copy.wait_recv()
    for copy in locals_:
        copy.wait()

    def project(i, _):
        cs = pl.ds(pl.multiple_of(i * 512, 512), 512)
        acc = stream[:, cs].astype(F32)
        for j in range(TP):
            acc = acc + dot(mix_in[j], ow_buf[j, :, cs])
        mid[:, cs] = acc.astype(BF16)
        return 0

    lax.fori_loop(0, D // 512, project, 0)

    own_set = jnp.where(heavy, 0, 1)

    def unit(s, dy, dx, h, dc=0):
        return (((s * 2 + (y + dy) % 2) * 2 + (x + dx) % 2) * 2 + h) * 2 + (c + dc) % 2

    NS = 32

    def norm(i, _):
        m = mid[pl.ds(pl.multiple_of(i * NS, NS), NS), :].astype(F32)
        scale = lax.rsqrt(jnp.mean(m * m, axis=-1, keepdims=True) + norm_eps)
        per = RH // NS
        rows[unit(own_set, 0, 0, i // per), pl.ds(pl.multiple_of(i % per * NS, NS), NS), :] = (
            m * scale * gain[...].reshape(1, D).astype(F32)
        ).astype(BF16)
        return 0

    lax.fori_loop(0, RT // NS, norm, 0)

    def piece(s, dy, dx, h, cut=None):
        if cut is None:
            return rows.at[unit(s, dy, dx, h)]
        return rows.at[unit(s, dy, dx, h), pl.ds(*cut), :]

    def pass_on(s, dy, dx, h, device, cut=None):
        return send(piece(s, dy, dx, h, cut), piece(s, dy, dx, h, cut), device)

    RQ = RH // 2
    whole = (0, RH)
    halves = ((0, RQ), (RQ, RQ))
    z_units = [
        (link(), u, cut)
        for u, cuts in (((0, 0, 0), (whole,)), ((0, 0, 1), (whole,)), ((0, 1, 0), halves), ((1, 0, 1), halves))
        for cut in cuts
    ]
    def links(many):
        count[0] += many
        return count[0] - many

    to_mate, to_x, to_y, to_last, to_done = (
        links(SLOTS), links(SLOTS), links(SLOTS), links(2 * N_CHUNKS), links(3)
    )
    ends_of = [k for k in range(N_CHUNKS) if chunk_at(k)[0]]
    common = list(pending)
    pending.clear()

    def cols_of(j):
        return pl.ds(pl.multiple_of(j * CB, CB), CB)

    def put(j, h, *terms):
        rs = pl.ds(h * RH, RH)
        acc = mid[rs, cols_of(j)].astype(F32)
        for term in terms:
            acc = acc + term.astype(F32)
        out[rs, cols_of(j)] = acc.astype(BF16)

    base = count[0]

    @pl.when(is_end)
    def _():
        sent = []

        def z_unit(i):
            k, (dy, dx, h), cut = z_units[i]
            start(k, piece(1, dy, dx, h, cut), piece(1, dy, dx, h, cut), dev(pz))

        side_x = pass_on(1, 0, 0, 0, x_dev)
        side_y = pass_on(1, 0, 0, 1, y_dev)
        down_first = send(down_half(oy, 0), down_at(z, y, 0), y_dev)
        z_unit(0)
        cross_last.wait_recv()
        up_send(z, oy, 1, up_at(z, oy, 1), goal_z, sent)
        z_unit(1)
        down_last = send(down_half(oy, 1), down_at(z, y, 1), y_dev)
        side_x.wait_recv()
        z_unit(2)
        z_unit(3)
        side_y.wait_recv()
        z_unit(4)
        z_unit(5)
        down_first.wait_recv()
        down_last.wait_recv()
        for yy in range(2):
            for i in range(2):
                down_send(z, yy, i, goal_z, sent)
        order = (pz, NZ - 1 - pz, z, NZ - 1 - z)
        done = []
        late = []

        def settle(limit):
            while late and late[0][0] <= limit:
                n, m, j = late.pop(0)
                arrive(to_done + m, z_done.at[m])
                for h in range(2):
                    put(j, h, z_done[m, h])

        for k in ends_of:
            _, n, last = chunk_kind(k)
            j = order[n // 2] * 2 + n % 2
            if last:
                late.append((n, n // 2, j))
                continue
            arrive(to_last + 2 * k, z_in.at[n, 0])
            a = send(z_in.at[n, 0, oy], last_in.at[k, 0], y_dev)
            arrive(to_last + 2 * k + 1, z_in.at[n, 1])
            b = send(z_in.at[n, 1, ox], last_in.at[k, 1], x_dev)
            if done:
                end_finish(done[-1], z_in, last_in, put, x, y)
            done.append((k, n, j, a, b))
            settle(n - 3)
        settle(SP)
        end_finish(done[-1], z_in, last_in, put, x, y)
        for copy in sent + pending:
            copy.wait_send()
        pending.clear()

    count[0] = base

    @pl.when(heavy)
    def _():
        sent = []
        hands = {}

        def hand(s, dy, dx, h):
            hands[s, dy, dx, h] = pass_on(s, dy, dx, h, mate_dev)

        def z_arrive(i):
            k, (dy, dx, h), cut = z_units[i]
            arrive(k, piece(1, dy, dx, h, cut))
            return pass_on(1, dy, dx, h, x_dev if h else y_dev, cut)

        def up_relay(yy):
            for i in range(2):
                up_wait(pz, yy, i)
                up_send(pz, yy, i, up_at(pz, yy, i), mz, sent)

        xa = pass_on(0, 0, 0, 0, x_dev)
        yb = pass_on(0, 0, 0, 1, y_dev)
        xb = pass_on(0, 0, 0, 1, x_dev)
        ya = pass_on(0, 0, 0, 0, y_dev)
        down_first = send(down_half(oy, 0), down_at(z, y, 0), y_dev)
        hand(0, 0, 0, 0)
        hand(0, 0, 0, 1)
        cross_last.wait_recv()
        up_send(z, oy, 1, up_at(z, oy, 1), goal_z, sent)
        up_relay(y)
        xa.wait_recv()
        corner_a = [pass_on(0, 0, 1, 0, y_dev, halves[0])]
        down_last = send(down_half(oy, 1), down_at(z, y, 1), y_dev)
        hand(0, 0, 1, 0)
        yb.wait_recv()
        corner_b = pass_on(0, 1, 0, 1, x_dev)
        hand(0, 1, 0, 1)
        ends = {}
        ends[1, 0, 0] = z_arrive(0)
        hand(1, 0, 0, 0)
        up_relay(oy)
        down_send(z, y, 0, mz, sent)
        down_send(z, y, 1, mz, sent)
        xb.wait_recv()
        hand(0, 0, 1, 1)
        ya.wait_recv()
        corner_a.append(pass_on(0, 1, 0, 0, x_dev, halves[1]))
        hand(0, 1, 0, 0)
        fz = NZ - 1 - pz

        def up_arrived(zs):
            for yy in range(2):
                for i in range(2):
                    up_wait(zs, yy, i)

        up_arrived(mz)

        KQ = D // NZ
        near_k = pl.ds(pl.multiple_of(jnp.where(fz == 0, KQ, 0), KQ), D - KQ)
        far_k = pl.ds(pl.multiple_of(fz * KQ, KQ), KQ)

        def handed(s, group):
            for dy, dx in group:
                for h in range(2):
                    hands[s, dy, dx, h].wait_recv()

        def over(group, one):
            first = group[0][0] * 2 + group[0][1]
            lax.fori_loop(first, first + len(group), one, 0)

        def chip(n):
            return (y + n // 2) % 2 * 2 + (x + n % 2) % 2

        def units_of(i):
            return pl.ds(pl.multiple_of(i * 4, 4), 4)

        def up_near(group):
            handed(0, group)

            def one(n, _):
                i = chip(n)
                up_sum[i] = dot(rows[units_of(i), :, near_k].reshape(2 * RT, D - KQ), up_buf[near_k, :])
                return 0

            over(group, one)

        def up_far(group):
            def one(n, _):
                i = chip(n)
                h = up_sum[i] + dot(rows[units_of(i), :, far_k].reshape(2 * RT, KQ), up_buf[far_k, :])
                h = jnp.maximum(h, 0.0)
                hidden[i] = (h * h).astype(BF16)
                return 0

            over(group, one)

        def up_rows(s, group):
            handed(s, group)

            def one(n, _):
                i = s * 4 + chip(n)
                h = jnp.maximum(dot(rows[units_of(i)].reshape(2 * RT, D), up_buf[...]), 0.0)
                hidden[i] = (h * h).astype(BF16)
                return 0

            over(group, one)

        slots = SLOTS

        def plane_of(i):
            if isinstance(i, int):
                return (z, mz, pz, NZ - 1 - pz)[i]
            return jnp.where(i == 0, z, jnp.where(i == 1, mz, jnp.where(i == 2, pz, NZ - 1 - pz)))

        def down_ready(i, yy):
            zs = (z, mz, pz, NZ - 1 - pz)[i]
            for h in range(2):
                down_wait(zs, yy, h)
                if i == 2:
                    relay_of(yy, h).start()

        relay_slots = [[z_slot() for _ in range(2)] for _ in range(2)]

        def relay_of(yy, h):
            ref = down_at(pz, yy, h)
            return z_copy(relay_slots[yy][h], down_sem(pz, yy, h), ref, ref, mz)

        def d_mate(k):
            return copy_of(to_mate + k % slots, part.at[k % slots, :, :, :, 1 - c], mate_in.at[k % slots], mate_dev)

        def d_x(k):
            return copy_of(to_x + k % slots, part.at[k % slots, :, ox, 0, c], x_in.at[k % slots], x_dev)

        def d_y(k):
            return copy_of(to_y + k % slots, part.at[k % slots, oy, :, 1, c], y_in.at[k % slots], y_dev)

        def d_last(k, h):
            src = part.at[k % slots, y, ox, 1, c] if h else part.at[k % slots, oy, x, 0, c]
            return copy_of(to_last + 2 * k + h, src, last_in.at[k, h], x_dev if h else y_dev)

        def d_through(k, h):
            src = part.at[k % slots, y, :, 1, c] if h else part.at[k % slots, :, x, 0, c]
            return copy_of(to_last + 2 * k + h, src, z_in.at[chunk_kind(k)[1], h], dev(pz))

        def d_done(k):
            m = chunk_kind(k)[1] // 2
            return copy_of(to_done + m, part.at[k % slots, y, x, :, c], z_done.at[m], dev(pz))

        def split(k, through, other):
            s, n, last = chunk_kind(k)
            if isinstance(k, int):
                (through if s and not last else other)()
            else:
                pl.when((s == 1) & jnp.logical_not(last))(through)
                pl.when((s == 0) | last)(other)

        def sent_all(k):
            d_mate(k).wait_send()
            d_x(k).wait_send()
            d_y(k).wait_send()

            def through():
                for h in range(2):
                    d_through(k, h).wait_send()

            def other():
                for h in range(2):
                    d_last(k, h).wait_send()

            split(k, through, other)

            @pl.when(chunk_kind(k)[2])
            def _():
                d_done(k).wait_send()

        def multiply(k):
            s, i, yy = chunk_at(k)
            j = plane_of(i) * 2 + yy
            got = dot(hidden[pl.ds(s * 4, 4)].reshape(8 * RT, FH), down_buf[j]).astype(BF16)
            part[k % slots] = got.reshape(2, 2, 2, 2, RH, CB)
            d_mate(k).start()

        def fold(k):
            slot = k % slots
            d_mate(k).wait_recv()

            def one(q, _):
                for h in range(2):
                    part[slot, q // 2, q % 2, h, c] = (
                        part[slot, q // 2, q % 2, h, c].astype(F32) + mate_in[slot, q // 2, q % 2, h].astype(F32)
                    ).astype(BF16)
                return 0

            lax.fori_loop(0, 4, one, 0)
            d_x(k).start()
            d_y(k).start()

        def spread(k):
            slot = k % slots
            d_x(k).wait_recv()
            for i in range(2):
                part[slot, i, x, 0, c] = (
                    part[slot, i, x, 0, c].astype(F32) + x_in[slot, i].astype(F32)
                ).astype(BF16)
            split(k, lambda: d_through(k, 0).start(), lambda: d_last(k, 0).start())
            d_y(k).wait_recv()
            for i in range(2):
                part[slot, y, i, 1, c] = (
                    part[slot, y, i, 1, c].astype(F32) + y_in[slot, i].astype(F32)
                ).astype(BF16)
            split(k, lambda: d_through(k, 1).start(), lambda: d_last(k, 1).start())

        def finish(k):
            s, n, last = chunk_kind(k)
            slot = k % slots
            j = plane_of(n // 2) * 2 + n % 2

            @pl.when(s == 0)
            def _():
                for h in range(2):
                    d_last(k, h).wait_recv()
                    put(j, h, part[slot, y, x, h, c], last_in[k, h])

            @pl.when(last)
            def _():
                for h in range(2):
                    d_last(k, h).wait_recv()
                    part[slot, y, x, h, c] = (
                        part[slot, y, x, h, c].astype(F32) + last_in[k, h].astype(F32)
                    ).astype(BF16)
                d_done(k).start()

        most = ((0, 0), (0, 1), (1, 0))
        far_corner = ((1, 1),)
        up_near(most)
        ends[0, 1, 1] = z_arrive(1)
        hand(1, 0, 0, 1)
        down_first.wait_recv()
        down_send(z, oy, 0, mz, sent)
        corner_b.wait_recv()
        hand(0, 1, 1, 1)
        for copy in corner_a:
            copy.wait_recv()
        hand(0, 1, 1, 0)
        ends[1, 1, 0] = [z_arrive(2), z_arrive(3)]
        hand(1, 0, 1, 0)
        up_near(far_corner)
        up_arrived(fz)
        up_far(most + far_corner)
        down_last.wait_recv()
        down_send(z, oy, 1, mz, sent)

        def lead(k, _):
            multiply(k)
            return 0

        ends[1, 1, 1] = [z_arrive(4)]
        lax.fori_loop(0, 2, lead, 0)
        up_rows(1, ((0, 0),))
        ends[1, 1, 1].append(z_arrive(5))
        hand(1, 1, 0, 1)
        fold(0)
        fold(1)
        ends[0, 1, 1].wait_recv()
        hand(1, 0, 1, 1)
        ends[1, 0, 0].wait_recv()
        hand(1, 1, 0, 0)
        up_rows(1, ((0, 1), (1, 0)))
        for copy in ends[1, 1, 1]:
            copy.wait_recv()
        hand(1, 1, 1, 1)
        for copy in ends[1, 1, 0]:
            copy.wait_recv()
        hand(1, 1, 1, 0)
        down_ready(1, 0)
        down_ready(1, 1)
        lax.fori_loop(2, 4, lead, 0)
        down_ready(2, 0)
        spread(0)
        up_rows(1, far_corner)
        fold(2)
        spread(1)

        def turn(k, _):
            pl.when(k >= 5)(lambda: finish(k - 5))
            pl.when((k >= 5) & (k < N_CHUNKS + 3))(lambda: spread(k - 3))
            pl.when(k < N_CHUNKS + 1)(lambda: fold(k - 1))
            for at, i, yy in ((6, 2, 1), (12, 3, 0), (13, 3, 1)):
                pl.when(k == at)(lambda i=i, yy=yy: down_ready(i, yy))
            pl.when((k >= slots) & (k < N_CHUNKS))(lambda: sent_all(k - slots))
            pl.when(k < N_CHUNKS)(lambda: multiply(k))
            return 0

        lax.fori_loop(OWN_LEAD, N_CHUNKS + 5, turn, 0)

        def drain(k, _):
            sent_all(k)
            return 0

        lax.fori_loop(N_CHUNKS - slots, N_CHUNKS, drain, 0)
        for yy in range(2):
            for h in range(2):
                relay_of(yy, h).wait_send()
        for copy in sent + pending:
            copy.wait_send()
        pending.clear()

    for when, copy in state_sends:
        @pl.when(when)
        def _(copy=copy):
            copy.wait_send()
    for copy in common + z_copies:
        copy.wait_send()


def end_finish(one, z_in, last_in, put, x, y):
    k, n, j, a, b = one
    a.wait_recv()
    put(j, 0, z_in[n, 0, y], last_in[k, 0])
    b.wait_recv()
    put(j, 1, z_in[n, 1, x], last_in[k, 1])


def one_kernel(SP, TP, *args):
    (stream, qw, kw, vw, gw, dw, qn, kn, vn, gn, dn, ow, on, gain, up, down) = args
    T = qw.shape[0]
    NB = T // BLOCK
    D = stream.shape[1]
    RT = T // TP
    RH = RT // 2
    FH = up.shape[1] // 2
    CB = down.shape[1]
    offs, starts = turn_tables(SP, T)
    vmem = pl.BlockSpec(memory_space=pltpu.VMEM)
    hbm = pl.BlockSpec(memory_space=pl.ANY)
    copies = 118
    return pl.pallas_call(
        functools.partial(layer_kernel, SP, TP),
        out_shape=jax.ShapeDtypeStruct((RT, D), BF16),
        in_specs=[vmem] * 14 + [hbm] * 4,
        out_specs=vmem,
        scratch_shapes=[
            pltpu.VMEM((D, FH), BF16),
            pltpu.VMEM((SP, FH, CB), BF16),
            pltpu.VMEM((TP, 256, D), BF16),
            pltpu.VMEM((7, 208, 128), BF16),
            pltpu.VMEM((T, 256), BF16),
            pltpu.VMEM((2, NB, 128, 128), F32),
            pltpu.VMEM((T, 256), F32),
            pltpu.VMEM((T, 256), BF16),
            pltpu.VMEM((TP, RT, 256), BF16),
            pltpu.VMEM((RT, D), BF16),
            pltpu.VMEM((32, RH, D), BF16),
            pltpu.VMEM((8, 2 * RT, FH), BF16),
            pltpu.VMEM((SLOTS, 2, 2, 2, 2, RH, CB), BF16),
            pltpu.VMEM((SLOTS, 2, 2, 2, RH, CB), BF16),
            pltpu.VMEM((SLOTS, 2, RH, CB), BF16),
            pltpu.VMEM((SLOTS, 2, RH, CB), BF16),
            pltpu.VMEM((2 * SP, 2, RH, CB), BF16),
            pltpu.VMEM((SP, 2, 2, RH, CB), BF16),
            pltpu.VMEM((3, 2, RH, CB), BF16),
            pltpu.VMEM((128, 128), F32),
            pltpu.VMEM((4, 2 * RT, FH), F32),
            pltpu.SemaphoreType.DMA((copies,)),
            pltpu.SemaphoreType.DMA((copies,)),
            pltpu.SemaphoreType.DMA((6,)),
            pltpu.SemaphoreType.DMA((22,)),
            pltpu.SemaphoreType.DMA((32,)),
            pltpu.SemaphoreType.DMA((4,)),
        ],
        compiler_params=pltpu.CompilerParams(
            collective_id=0, has_side_effects=True, vmem_limit_bytes=63 * 1024 * 1024
        ),
    )(stream, qw, kw, vw, gw, qn, kn, vn, gn, dw, dn, jnp.asarray(offs), jnp.asarray(starts),
      gain, ow, on, up, down)


def fits_kernel(SP, TP, args):
    D, FF = args[14].shape
    T = args[1].shape[0] // SP
    return (
        SP == 8 and TP == 4 and D % (SP * 128) == 0 and T % (TP * 32) == 0 and T % BLOCK == 0
        and args[1].shape[1] == TP * 128 and args[6].shape[1] == TP * 128
    )


def solution(mesh):
    in_specs = (
        P(("sp", "tp"), None),
        P("sp", "tp"),
        P("sp", "tp"),
        P("sp", "tp"),
        P("sp", "tp"),
        P("tp", "sp"),
        P("sp", "tp"),
        P("sp", "tp"),
        P("sp", "tp"),
        P("sp", "tp"),
        P("tp", "sp"),
        P("tp", None),
        P("tp", None),
        P(),
        P("sp", "tp"),
        P("tp", "sp"),
    )
    out_specs = P(("sp", "tp"), None)
    SP, TP = mesh.shape["sp"], mesh.shape["tp"]

    def layer(*args):
        body = functools.partial(one_kernel, SP, TP) if fits_kernel(SP, TP, args) else on_device
        return jax.shard_map(
            body, mesh=mesh, in_specs=in_specs, out_specs=out_specs, check_vma=False
        )(*args)

    return layer
```

```python
import functools
import jax
import jax.numpy as jnp
import numpy as np
from jax import lax
from jax.experimental import pallas as pl
from jax.experimental.pallas import tpu as pltpu
from jax.sharding import PartitionSpec as P

HDW = 128
HDN = 64
BLOCK = 128


head_eps = 1e-05
norm_eps = 1e-06
rope_base = 10000.0


def carried_in(shard, axis, join, neutral):
    place = lax.axis_index(axis)
    gathered = jax.tree.map(
        lambda a, kind: lax.all_gather(a.astype(kind), axis),
        shard,
        (jnp.bfloat16, jnp.bfloat16, jnp.bfloat16, jnp.bfloat16),
    )
    state = jax.tree.map(lambda a, e: jnp.zeros_like(a) + jnp.asarray(e, a.dtype), shard, neutral)

    def one(turn, state):
        return join(
            state,
            jax.tree.map(
                lambda a, own: lax.dynamic_index_in_dim(a, turn, 0, False).astype(own.dtype),
                gathered,
                shard,
            ),
        )

    return lax.fori_loop(0, place, one, state)


def rotate(values, places):
    half = values.shape[-1] // 2
    inverse = rope_base ** (-jnp.arange(half, dtype=jnp.float32) / half)
    angles = places[:, None] * inverse[None, :]
    cosine = jnp.cos(angles)[:, None, :]
    sine = jnp.sin(angles)[:, None, :]
    front = values[..., :half]
    back = values[..., half:]
    return jnp.concatenate([front * cosine - back * sine, back * cosine + front * sine], axis=-1)


def block_step(carried, inputs):
    query, keys, values, log_rate = inputs
    running = jnp.cumsum(log_rate, axis=0)
    spread = running[:, None, :] - running[None, :, :]
    length = log_rate.shape[0]
    lower = (jnp.arange(length)[:, None] >= jnp.arange(length)[None, :])[:, :, None]
    factor = jnp.where(lower, jnp.exp(jnp.minimum(spread, 0.0)), 0.0)
    scores = jnp.einsum("thd,shd->tsh", query, keys) * factor
    within = jnp.einsum("tsh,she->the", scores, values)
    across = jnp.einsum("thd,hde->the", query, carried) * jnp.exp(running)[:, :, None]
    tail_decay = jnp.exp(running[-1][None, :] - running)
    updated = jnp.exp(running[-1])[:, None, None] * carried + jnp.einsum(
        "shd,she->hde", keys * tail_decay[:, :, None], values
    )
    return (updated, within + across)


def head_norm(values):
    centre = values - jnp.mean(values, axis=-1, keepdims=True)
    spread = jnp.mean(centre * centre, axis=-1, keepdims=True)
    return centre * lax.rsqrt(spread + head_eps)


def local_group(query, keys, values, log_rate, width, places):
    length = query.shape[0]
    count_of_heads = query.shape[1] // width
    blocks = length // BLOCK

    def split(array):
        return array.astype(jnp.float32).reshape(length, count_of_heads, width)

    query_rot = rotate(split(query), places)
    keys_rot = rotate(split(keys), places) * width ** (-0.5)
    rates = log_rate.T
    carried = jnp.zeros((count_of_heads, width, width), jnp.float32)
    final_state, outputs = lax.scan(
        block_step,
        carried,
        (
            query_rot.reshape(blocks, BLOCK, count_of_heads, width),
            keys_rot.reshape(blocks, BLOCK, count_of_heads, width),
            split(values).reshape(blocks, BLOCK, count_of_heads, width),
            rates.reshape(blocks, BLOCK, count_of_heads),
        ),
    )
    running = jnp.cumsum(rates, axis=0)
    return (
        query_rot,
        outputs.reshape(length, count_of_heads, width),
        final_state,
        jnp.exp(running[-1]),
        running,
    )


def finish_group(query_rot, outputs, incoming, running, gate):
    length = outputs.shape[0]
    outputs = (
        outputs + jnp.einsum("thd,hde->the", query_rot, incoming) * jnp.exp(running)[:, :, None]
    )
    normed = head_norm(outputs).reshape(length, -1)
    return (jax.nn.silu(gate.astype(jnp.float32)) * normed).astype(jnp.bfloat16)


def chain(earlier, later):
    rate_wide, memory_wide, rate_narrow, memory_narrow = earlier
    later_rate_wide, later_memory_wide, later_rate_narrow, later_memory_narrow = later
    return (
        rate_wide * later_rate_wide,
        memory_wide * later_rate_wide[:, None, None] + later_memory_wide,
        rate_narrow * later_rate_narrow,
        memory_narrow * later_rate_narrow[:, None, None] + later_memory_narrow,
    )


def row_norm(middle, norm_gain):
    middle_f = middle.astype(jnp.float32)
    scale = lax.rsqrt(jnp.mean(middle_f * middle_f, axis=-1, keepdims=True) + norm_eps)
    return (middle_f * scale * norm_gain.astype(jnp.float32)).astype(jnp.bfloat16)


def on_device(
    stream_in,
    query_wide,
    key_wide,
    value_wide,
    gate_wide,
    decay_wide,
    query_narrow,
    key_narrow,
    value_narrow,
    gate_narrow,
    decay_narrow,
    output_wide,
    output_narrow,
    norm_gain,
    up_weight,
    down_weight,
):
    length = query_wide.shape[0]
    places = (lax.axis_index("sp") * length + jnp.arange(length, dtype=jnp.int32)).astype(
        jnp.float32
    )
    wide_query, wide_out, wide_state, wide_total, wide_running = local_group(
        query_wide, key_wide, value_wide, decay_wide, HDW, places
    )
    narrow_query, narrow_out, narrow_state, narrow_total, narrow_running = local_group(
        query_narrow, key_narrow, value_narrow, decay_narrow, HDN, places
    )
    identity = (
        jnp.ones_like(wide_total),
        jnp.zeros_like(wide_state),
        jnp.ones_like(narrow_total),
        jnp.zeros_like(narrow_state),
    )
    incoming = carried_in(
        (wide_total, wide_state, narrow_total, narrow_state), "sp", chain, identity
    )
    mixed_wide = finish_group(wide_query, wide_out, incoming[1], wide_running, gate_wide)
    mixed_narrow = finish_group(narrow_query, narrow_out, incoming[3], narrow_running, gate_narrow)
    mixed_sum = lax.psum_scatter(
        (
            jnp.dot(mixed_wide, output_wide, preferred_element_type=jnp.float32)
            + jnp.dot(mixed_narrow, output_narrow, preferred_element_type=jnp.float32)
        ).astype(jnp.bfloat16),
        "tp",
        scatter_dimension=0,
        tiled=True,
    ).astype(jnp.float32)
    middle = (stream_in.astype(jnp.float32) + mixed_sum).astype(jnp.bfloat16)
    normed = lax.all_gather(row_norm(middle, norm_gain), "tp", axis=0, tiled=True)
    up_sum = jnp.dot(
        normed,
        lax.all_gather(up_weight, "sp", axis=0, tiled=True),
        preferred_element_type=jnp.float32,
    )
    hidden = jnp.square(jax.nn.relu(up_sum)).astype(jnp.bfloat16)
    down_sum = jnp.dot(
        hidden,
        lax.all_gather(down_weight, "sp", axis=1, tiled=True),
        preferred_element_type=jnp.float32,
    )
    down_rows = lax.psum_scatter(
        down_sum.astype(jnp.bfloat16), "tp", scatter_dimension=0, tiled=True
    ).astype(jnp.float32)
    return (middle.astype(jnp.float32) + down_rows).astype(jnp.bfloat16)


F32 = jnp.float32
BF16 = jnp.bfloat16
MESH_ID = pl.DeviceIdType.MESH


def turn_tables(shards, length):
    lane = np.arange(128)
    offsets, starts = [], []
    for width in (HDW, HDN):
        half = width // 2
        inverse = rope_base ** (-((lane % half).astype(np.float64)) / half)
        inside = np.arange(BLOCK)[:, None] * inverse[None, :]
        first = (np.arange(shards * length // BLOCK) * BLOCK)[:, None] * inverse[None, :]
        offsets += [np.cos(inside), np.sin(inside)]
        starts += [np.cos(first), np.sin(first)]
    return np.stack(offsets).astype(np.float32), np.stack(starts).astype(np.float32)


def dot(a, b):
    return jnp.dot(a, b, preferred_element_type=F32)


def dot_rows(a, b):
    return lax.dot_general(a, b, (((0,), (0,)), ((), ())), preferred_element_type=F32)


def dot_cols(a, b):
    return lax.dot_general(a, b, (((1,), (1,)), ((), ())), preferred_element_type=F32)


N_CHUNKS = 16
OWN_LEAD = 4
SLOTS = 8


def chunk_at(k):
    t = k - OWN_LEAD
    if isinstance(k, int):
        if t < 0:
            return 0, k // 2, k % 2
        far = t % 3 != 2 if t < 8 else t < 10
        n = (t - t // 3 if far else 4 + t // 3) if t < 8 else (t - 2 if far else t - 4)
        return int(far), n // 2, n % 2
    far = jnp.where(t < 8, jnp.where(t % 3 != 2, 1, 0), jnp.where(t < 10, 1, 0)) == 1
    early = jnp.where(far, t - t // 3, 4 + t // 3)
    n = jnp.where(t < 0, k, jnp.where(t < 8, early, jnp.where(far, t - 2, t - 4)))
    return jnp.where((t >= 0) & far, 1, 0), n // 2, n % 2


def chunk_kind(k):
    s, i, yy = chunk_at(k)
    n = i * 2 + yy
    last = (s == 1) & (yy == 1) & (i > 0)
    return s, n, last


def layer_kernel(
    SP, TP,
    kw, vw, kn, vn, dw, dn, offs, starts, gain, stream_at, qw_at, qn_at, gw_at, gn_at, ow_w, ow_n, up, down,
    out_at,
    up_buf, down_buf, ow_buf, st_buf, k_rot, before, inside, mixed, mix_in, mid, rows, hidden, part,
    mate_in, x_in, y_in, last_in, z_in, z_done, rates_buf, up_sum, stream, qw, qn, gw, gn, out,
    ssem, rsem, lsem, zsend, zrecv, srecv, osem,
):
    sp = lax.axis_index("sp")
    tp = lax.axis_index("tp")
    NZ = SP // 2
    z, y = sp // 2, sp % 2
    x, c = tp // 2, tp % 2
    T = kw.shape[0]
    NB = T // BLOCK
    RT = T // TP
    RH = RT // 2
    RB = up.shape[0]
    CB = down.shape[1]
    D = up_buf.shape[0]
    FH = up.shape[1] // 2
    heavy = (z == 1) | (z == 2)
    is_end = jnp.logical_not(heavy)
    pz = z + 1 - 2 * (z % 2)
    mz = NZ - 1 - z
    goal_z = jnp.where(heavy, mz, pz)

    def dev(zz, dy=0, dx=0, dc=0):
        return (zz * 2 + (y + dy) % 2, (x + dx) % 2 * 2 + (c + dc) % 2)

    x_dev, y_dev, mate_dev = dev(z, 0, 1), dev(z, 1), dev(z, 0, 0, 1)
    count = [0]
    pending = []

    def link():
        count[0] += 1
        return count[0] - 1

    def copy_of(k, src, dst, device, ks=None):
        return pltpu.make_async_remote_copy(
            src_ref=src, dst_ref=dst, send_sem=ssem.at[k if ks is None else ks], recv_sem=rsem.at[k],
            device_id=device, device_id_type=MESH_ID,
        )

    def start(k, src, dst, device):
        copy = copy_of(k, src, dst, device)
        copy.start()
        pending.append(copy)
        return copy

    def send(src, dst, device):
        return start(link(), src, dst, device)

    def arrive(k, dst):
        copy_of(k, dst, dst, mate_dev).wait_recv()

    locals_ = []

    def keep(src, dst):
        copy = pltpu.make_async_copy(src, dst, lsem.at[len(locals_)])
        copy.start()
        locals_.append(copy)
        return copy

    barrier = pltpu.get_barrier_semaphore()
    for d in range(1, NZ):
        pl.semaphore_signal(barrier, inc=1, device_id=dev((z + d) % NZ), device_id_type=MESH_ID)
    for device in (x_dev, y_dev, mate_dev, dev(z, 0, 1, 1)):
        pl.semaphore_signal(barrier, inc=1, device_id=device, device_id_type=MESH_ID)
    for src, dst in ((qw_at, qw), (qn_at, qn), (gw_at, gw), (gn_at, gn), (stream_at, stream)):
        keep(src, dst)
    pl.semaphore_wait(barrier, NZ + 3)

    HB = RB // 2
    HF = FH // 2

    def up_at(zs, yy, part_of):
        return up_buf.at[pl.ds(pl.multiple_of((zs * 2 + yy) * RB + part_of * HB, HB), HB), :]

    def down_at(zs, yy, part_of):
        return down_buf.at[zs * 2 + yy, pl.ds(part_of * HF, HF), :]

    def up_half(half, part_of):
        return up.at[pl.ds(part_of * HB, HB), pl.ds(pl.multiple_of(half * FH, FH), FH)]

    def down_half(half, part_of):
        return down.at[pl.ds(pl.multiple_of(half * FH + part_of * HF, HF), HF), :]

    z_copies = []

    def z_copy(slot, sem, src, dst, zz):
        return pltpu.make_async_remote_copy(
            src_ref=src, dst_ref=dst, send_sem=zsend.at[slot], recv_sem=zrecv.at[sem],
            device_id=dev(zz), device_id_type=MESH_ID,
        )

    def up_sem(zs, yy, part_of):
        return (zs * 2 + yy) * 2 + part_of

    def down_sem(zs, yy, part_of):
        return 4 * NZ + up_sem(zs, yy, part_of)

    z_slots = [0]

    def z_slot():
        z_slots[0] += 1
        return z_slots[0] - 1

    def up_send(zs, yy, part_of, src, zz, into):
        copy = z_copy(z_slot(), up_sem(zs, yy, part_of), src, up_at(zs, yy, part_of), zz)
        copy.start()
        into.append(copy)

    def down_send(zs, yy, part_of, zz, into):
        ref = down_at(zs, yy, part_of)
        copy = z_copy(z_slot(), down_sem(zs, yy, part_of), ref, ref, zz)
        copy.start()
        into.append(copy)

    def up_wait(zs, yy, part_of):
        ref = up_at(zs, yy, part_of)
        z_copy(0, up_sem(zs, yy, part_of), ref, ref, goal_z).wait_recv()

    def down_wait(zs, yy, part_of):
        ref = down_at(zs, yy, part_of)
        z_copy(0, down_sem(zs, yy, part_of), ref, ref, goal_z).wait_recv()

    oy = 1 - y
    ox = 1 - x
    RW = D * 3 // 8
    QB = HB // 4

    def ow_at(i, g, cols):
        return ow_buf.at[i, pl.ds(g * 128, 128), cols]

    def relay_cols(yy):
        return pl.ds(pl.multiple_of(yy * (D - RW), 128), RW)

    main_cols = pl.ds(RW, D - 2 * RW)
    every = pl.ds(0, D)
    side = ox * 2 + c
    ow_first = [
        send(r.at[:, relay_cols(y)], ow_at(tp, g, relay_cols(y)), x_dev) for g, r in enumerate((ow_w, ow_n))
    ]
    ow_main = [
        send(r.at[:, main_cols], ow_at(tp, g, main_cols), x_dev) for g, r in enumerate((ow_w, ow_n))
    ]
    ow_mate = [send(r, ow_at(tp, g, every), mate_dev) for g, r in enumerate((ow_w, ow_n))]
    up_send(z, y, 0, up_half(y, 0), goal_z, z_copies)
    keep(ow_w, ow_at(tp, 0, every))
    keep(ow_n, ow_at(tp, 1, every))
    keep(up_half(y, 0), up_at(z, y, 0))
    keep(up_half(y, 1), up_at(z, y, 1))
    for i in range(2):
        keep(down_half(y, i), down_at(z, y, i))

    def cross_rows(first, many):
        return send(
            up.at[pl.ds(first, many), pl.ds(pl.multiple_of(oy * FH, FH), FH)],
            up_buf.at[pl.ds(pl.multiple_of(sp * RB + first, QB), many), :], y_dev,
        )

    cross_first = [cross_rows(0, QB)]

    lane = lax.broadcasted_iota(jnp.int32, (128, 128), 1)
    row = lax.broadcasted_iota(jnp.int32, (128, 128), 0)
    lower = row >= lane
    low = lane < HDN
    low_row = row < HDN
    low_half = lax.broadcasted_iota(jnp.int32, (HDN, 128), 1) < HDN
    diagonal = low == low_row
    for h in range(3):
        for b in range(NB):
            ref = dw if h == 0 else dn
            at = 0 if h == 0 else h - 1
            rates_buf[h * NB + b:h * NB + b + 1, :] = ref[at:at + 1, b * BLOCK:(b + 1) * BLOCK]
    cr = rates_buf[...]
    step = 1
    while step < 128:
        cr = cr + jnp.where(lane >= step, pltpu.roll(cr, step, 1), 0.0)
        step *= 2
    ct = cr.T

    def col(h, b):
        return ct[:, h * NB + b:h * NB + b + 1]

    def line(h, b):
        return cr[h * NB + b:h * NB + b + 1, :]

    def total(h, b):
        return cr[h * NB + b:h * NB + b + 1, 127:128]

    def pair(a, b):
        return jnp.where(low, a, b)

    sign_w = jnp.where(low, -1.0, 1.0)
    early = (lane % HDN) < HDN // 2
    sign_n = jnp.where(early, -1.0, 1.0)

    def tables(g, b):
        cb = starts[2 * g, pl.ds(sp * NB + b, 1), :]
        sb = starts[2 * g + 1, pl.ds(sp * NB + b, 1), :]
        co, so = offs[2 * g], offs[2 * g + 1]
        return co * cb - so * sb, (so * cb + co * sb) * (sign_n if g else sign_w)

    def turned(v, table, g):
        if g:
            other = jnp.where(early, pltpu.roll(v, 128 - HDN // 2, 1), pltpu.roll(v, HDN // 2, 1))
        else:
            other = pltpu.roll(v, HDW // 2, 1)
        return v * table[0] + other * table[1]

    state_w = jnp.zeros((128, 128), F32)
    state_n = jnp.zeros((128, 128), F32)
    sums = [jnp.zeros((1, 1), F32) for _ in range(3)]
    for b in range(NB):
        rs = pl.ds(b * BLOCK, BLOCK)
        before[0, b] = state_w
        before[1, b] = state_n
        kwr = turned(kw[rs, :].astype(F32), tables(0, b), 0) * HDW ** (-0.5)
        knr = turned(kn[rs, :].astype(F32), tables(1, b), 1) * HDN ** (-0.5)
        k_rot[rs, 0:128] = kwr.astype(BF16)
        k_rot[rs, 128:256] = knr.astype(BF16)
        t0, t1, t2 = total(0, b), total(1, b), total(2, b)
        sums = [s + t for s, t in zip(sums, (t0, t1, t2))]
        tail_w = jnp.exp(t0 - col(0, b))
        tail_n = pair(jnp.exp(t1 - col(1, b)), jnp.exp(t2 - col(2, b)))
        state_w = jnp.exp(t0) * state_w + dot_rows((kwr * tail_w).astype(BF16), vw[rs, :])
        grown = dot_rows((knr * tail_n).astype(BF16), vn[rs, :])
        state_n = jnp.where(low_row, jnp.exp(t1), jnp.exp(t2)) * state_n + jnp.where(diagonal, grown, 0.0)
    small = lax.broadcasted_iota(jnp.int32, (16, 128), 0)
    rates = jnp.where(small == 0, jnp.exp(sums[0]), jnp.where(small == 1, jnp.exp(sums[1]), jnp.exp(sums[2])))
    st_buf[0, 0:128, :] = state_w.astype(BF16)
    st_buf[0, 128:192, :] = (state_n[0:HDN, :] + state_n[HDN:128, :]).astype(BF16)
    st_buf[0, 192:208, :] = rates.astype(BF16)
    state_y = send(st_buf.at[0], st_buf.at[1], y_dev)
    cross_first.append(cross_rows(QB, HB - QB))

    for copy in locals_[:2]:
        copy.wait()
    for b in range(NB):
        rs = pl.ds(b * BLOCK, BLOCK)
        kwr, knr = k_rot[rs, 0:128], k_rot[rs, 128:256]
        qwr = turned(qw[rs, :].astype(F32), tables(0, b), 0)
        qnr = turned(qn[rs, :].astype(F32), tables(1, b), 1)

        def factor(h):
            return jnp.where(lower, jnp.exp(jnp.minimum(col(h, b) - line(h, b), 0.0)), 0.0)

        scores = (dot_cols(qwr.astype(BF16), kwr) * factor(0)).astype(BF16)
        inside[rs, 0:128] = dot(scores, vw[rs, :])
        near = (dot_cols(jnp.where(low, qnr, 0.0).astype(BF16), knr) * factor(1)).astype(BF16)
        far = (dot_cols(jnp.where(low, 0.0, qnr).astype(BF16), knr) * factor(2)).astype(BF16)
        inside[rs, 128:256] = pair(dot(near, vn[rs, :]), dot(far, vn[rs, :]))
        k_rot[rs, 0:128] = (qwr * jnp.exp(col(0, b))).astype(BF16)
        k_rot[rs, 128:256] = (qnr * pair(jnp.exp(col(1, b)), jnp.exp(col(2, b)))).astype(BF16)

    def state(i):
        return st_buf[i, 0:128, :].astype(F32), st_buf[i, 128:192, :].astype(F32), st_buf[i, 192:208, :].astype(F32)

    def chained(first, second):
        r = second[2]
        return (
            first[0] * r[0:1, :] + second[0],
            first[1] * jnp.where(low_half, r[1:2, :], r[2:3, :]) + second[1],
            first[2] * r,
        )

    state_y.wait_recv()
    mine, theirs = state(0), state(1)
    lead = [jnp.where(y == 0, a, b) for a, b in zip(mine, theirs)]
    rear = [jnp.where(y == 0, b, a) for a, b in zip(mine, theirs)]
    plane = chained(lead, rear)
    st_buf[2, 0:128, :] = plane[0].astype(BF16)
    st_buf[2, 128:192, :] = plane[1].astype(BF16)
    st_buf[2, 192:208, :] = plane[2].astype(BF16)

    def state_copy(k, zs, zz):
        return pltpu.make_async_remote_copy(
            src_ref=st_buf.at[2], dst_ref=st_buf.at[3 + zs], send_sem=ssem.at[k], recv_sem=srecv.at[zs],
            device_id=dev(zz), device_id_type=MESH_ID,
        )

    state_sends = []
    for d in range(NZ - 1, 0, -1):
        copy = state_copy(link(), z, (z + d) % NZ)
        state_sends.append((z + d < NZ, copy))

        @pl.when(z + d < NZ)
        def _(copy=copy):
            copy.start()

    up_send(z, y, 1, up_half(y, 1), goal_z, z_copies)
    ow_y = []
    for g, copy in enumerate(ow_first):
        copy.wait_recv()
        ow_y.append(send(ow_at(side, g, relay_cols(y)), ow_at(side, g, relay_cols(y)), y_dev))
    cross_last = send(up_half(oy, 1), up_at(z, y, 1), y_dev)
    ow_hand = [send(ow_buf.at[side, :, relay_cols(y)], ow_buf.at[side, :, relay_cols(y)], mate_dev)]

    for copy in cross_first:
        copy.wait_recv()
    up_send(z, oy, 0, up_at(z, oy, 0), goal_z, z_copies)
    for zs in range(NZ - 1):
        @pl.when(zs < z)
        def _(zs=zs):
            state_copy(0, zs, mz).wait_recv()

    held = (jnp.zeros((128, 128), F32), jnp.zeros((HDN, 128), F32), jnp.zeros((16, 128), F32))
    for zs in range(NZ - 1):
        held = [jnp.where(zs < z, a, b) for a, b in zip(chained(held, state(3 + zs)), held)]
    held = [jnp.where(y == 1, a, b) for a, b in zip(chained(held, theirs), held)]
    s_w = held[0]
    s_n = jnp.concatenate([jnp.where(low_half, held[1], 0.0), jnp.where(low_half, 0.0, held[1])], axis=0)

    for copy in locals_[2:4]:
        copy.wait()
    sums = [jnp.zeros((1, 1), F32) for _ in range(3)]
    for b in range(NB):
        rs = pl.ds(b * BLOCK, BLOCK)
        whole_w = before[0, b] + jnp.exp(sums[0]) * s_w
        whole_n = before[1, b] + jnp.where(low_row, jnp.exp(sums[1]), jnp.exp(sums[2])) * s_n
        sums = [s + total(h, b) for h, s in enumerate(sums)]
        o_w = inside[rs, 0:128] + dot(k_rot[rs, 0:128], whole_w.astype(BF16))
        o_n = inside[rs, 128:256] + dot(k_rot[rs, 128:256], whole_n.astype(BF16))

        def both(v):
            first = jnp.sum(jnp.where(low, v, 0.0), axis=-1, keepdims=True) / HDN
            second = jnp.sum(jnp.where(low, 0.0, v), axis=-1, keepdims=True) / HDN
            return pair(first, second)

        c_w = o_w - jnp.mean(o_w, axis=-1, keepdims=True)
        n_w = c_w * lax.rsqrt(jnp.mean(c_w * c_w, axis=-1, keepdims=True) + head_eps)
        c_n = o_n - both(o_n)
        n_n = c_n * lax.rsqrt(both(c_n * c_n) + head_eps)
        mixed[rs, 0:128] = (jax.nn.silu(gw[rs, :].astype(F32)) * n_w).astype(BF16)
        mixed[rs, 128:256] = (jax.nn.silu(gn[rs, :].astype(F32)) * n_n).astype(BF16)

    def my_rows(i):
        return pl.ds(pl.multiple_of(i * RT, RT), RT)

    swaps = [
        send(mixed.at[my_rows((x + dx) % 2 * 2 + (c + dc) % 2), :], mix_in.at[tp], dev(z, 0, dx, dc))
        for dx, dc in ((1, 0), (1, 1), (0, 1))
    ]
    mix_in[tp] = mixed[my_rows(tp), :]
    for copy in ow_main:
        copy.wait_recv()
    ow_hand.append(send(ow_buf.at[side, :, main_cols], ow_buf.at[side, :, main_cols], mate_dev))
    for copy in ow_y:
        copy.wait_recv()
    ow_hand.append(send(ow_buf.at[side, :, relay_cols(oy)], ow_buf.at[side, :, relay_cols(oy)], mate_dev))
    for copy in ow_mate + ow_hand + swaps:
        copy.wait_recv()
    for copy in locals_[4:]:
        copy.wait()

    def project(i, _):
        cs = pl.ds(pl.multiple_of(i * 512, 512), 512)
        acc = stream[:, cs].astype(F32)
        for j in range(TP):
            acc = acc + dot(mix_in[j], ow_buf[j, :, cs])
        mid[:, cs] = acc.astype(BF16)
        return 0

    lax.fori_loop(0, D // 512, project, 0)

    own_set = jnp.where(heavy, 0, 1)

    def unit(s, dy, dx, h, dc=0):
        return (((s * 2 + (y + dy) % 2) * 2 + (x + dx) % 2) * 2 + h) * 2 + (c + dc) % 2

    NS = 32

    def norm(i, _):
        m = mid[pl.ds(pl.multiple_of(i * NS, NS), NS), :].astype(F32)
        scale = lax.rsqrt(jnp.mean(m * m, axis=-1, keepdims=True) + norm_eps)
        per = RH // NS
        rows[unit(own_set, 0, 0, i // per), pl.ds(pl.multiple_of(i % per * NS, NS), NS), :] = (
            m * scale * gain[...].reshape(1, D).astype(F32)
        ).astype(BF16)
        return 0

    lax.fori_loop(0, RT // NS, norm, 0)

    def piece(s, dy, dx, h, cut=None):
        if cut is None:
            return rows.at[unit(s, dy, dx, h)]
        return rows.at[unit(s, dy, dx, h), pl.ds(*cut), :]

    def pass_on(s, dy, dx, h, device, cut=None):
        return send(piece(s, dy, dx, h, cut), piece(s, dy, dx, h, cut), device)

    RQ = RH // 2
    whole = (0, RH)
    halves = ((0, RQ), (RQ, RQ))
    thirds = ((0, RH // 3), (RH // 3, RH - RH // 3))
    z_units = [
        (link(), u, cut)
        for u, cuts in (((0, 0, 0), (whole,)), ((0, 0, 1), (whole,)), ((0, 1, 0), halves), ((1, 0, 1), halves))
        for cut in cuts
    ]
    def links(many):
        count[0] += many
        return count[0] - many

    to_mate, to_x, to_y, to_last, to_done = (
        links(SLOTS), links(SLOTS), links(SLOTS), links(2 * SLOTS), links(3)
    )
    ends_of = [k for k in range(N_CHUNKS) if chunk_at(k)[0]]
    common = list(pending)
    pending.clear()

    def cols_of(j):
        return pl.ds(pl.multiple_of(j * CB, CB), CB)

    def put(j, h, *terms):
        rs = pl.ds(h * RH, RH)
        acc = mid[rs, cols_of(j)].astype(F32)
        for term in terms:
            acc = acc + term.astype(F32)
        out[rs, cols_of(j)] = acc.astype(BF16)

    base = count[0]

    def put_out(j):
        pltpu.make_async_copy(out.at[:, cols_of(j)], out_at.at[:, cols_of(j)], osem).start()

    @pl.when(is_end)
    def _():
        sent = []

        def z_unit(i):
            k, (dy, dx, h), cut = z_units[i]
            start(k, piece(1, dy, dx, h, cut), piece(1, dy, dx, h, cut), dev(pz))

        side_x = pass_on(1, 0, 0, 0, x_dev)
        side_y = pass_on(1, 0, 0, 1, y_dev)
        down_first = send(down_half(oy, 0), down_at(z, y, 0), y_dev)
        z_unit(0)
        cross_last.wait_recv()
        up_send(z, oy, 1, up_at(z, oy, 1), goal_z, sent)
        z_unit(1)
        down_last = send(down_half(oy, 1), down_at(z, y, 1), y_dev)
        side_x.wait_recv()
        z_unit(2)
        z_unit(3)
        side_y.wait_recv()
        z_unit(4)
        z_unit(5)
        down_first.wait_recv()
        down_last.wait_recv()
        for yy in range(2):
            for i in range(2):
                down_send(z, yy, i, goal_z, sent)
        order = (pz, NZ - 1 - pz, z, NZ - 1 - z)
        done = []
        late = []

        def settle(limit):
            while late and late[0][0] <= limit:
                n, m, j = late.pop(0)
                arrive(to_done + m, z_done.at[m])
                for h in range(2):
                    put(j, h, z_done[m, h])
                put_out(j)

        for k in ends_of:
            _, n, last = chunk_kind(k)
            j = order[n // 2] * 2 + n % 2
            if last:
                late.append((n, n // 2 - 1, j))
                continue
            arrive(to_last + 2 * n, z_in.at[n, 0])
            a = send(z_in.at[n, 0, oy], last_in.at[k, 0], y_dev)
            arrive(to_last + 2 * n + 1, z_in.at[n, 1])
            b = send(z_in.at[n, 1, ox], last_in.at[k, 1], x_dev)
            if done:
                end_finish(done[-1], z_in, last_in, put, put_out, x, y)
            done.append((k, n, j, a, b))
            settle(n - 3)
        settle(SP)
        end_finish(done[-1], z_in, last_in, put, put_out, x, y)
        for copy in sent + pending:
            copy.wait_send()
        pending.clear()

    count[0] = base

    @pl.when(heavy)
    def _():
        sent = []
        hand_send = link()
        hand_first = links(8)

        def hand(s, dy, dx, h):
            ref = piece(s, dy, dx, h)
            copy_of(hand_first + (s * 2 + dy) * 2 + dx, ref, ref, mate_dev, hand_send).start()

        def z_arrive(i):
            k, (dy, dx, h), cut = z_units[i]
            arrive(k, piece(1, dy, dx, h, cut))
            return pass_on(1, dy, dx, h, x_dev if h else y_dev, cut)

        def up_relay(yy):
            for i in range(2):
                up_wait(pz, yy, i)
                up_send(pz, yy, i, up_at(pz, yy, i), mz, sent)

        xa = pass_on(0, 0, 0, 0, x_dev)
        yb = pass_on(0, 0, 0, 1, y_dev)
        xb = pass_on(0, 0, 0, 1, x_dev)
        ya = pass_on(0, 0, 0, 0, y_dev)
        down_first = send(down_half(oy, 0), down_at(z, y, 0), y_dev)
        hand(0, 0, 0, 0)
        hand(0, 0, 0, 1)
        cross_last.wait_recv()
        up_send(z, oy, 1, up_at(z, oy, 1), goal_z, sent)
        up_relay(y)
        xa.wait_recv()
        corner_a = [pass_on(0, 0, 1, 0, y_dev, thirds[0])]
        down_last = send(down_half(oy, 1), down_at(z, y, 1), y_dev)
        hand(0, 0, 1, 0)
        yb.wait_recv()
        corner_b = pass_on(0, 1, 0, 1, x_dev)
        hand(0, 1, 0, 1)
        ends = {}
        ends[1, 0, 0] = z_arrive(0)
        hand(1, 0, 0, 0)
        up_relay(oy)
        down_send(z, y, 0, mz, sent)
        down_send(z, y, 1, mz, sent)
        xb.wait_recv()
        hand(0, 0, 1, 1)
        ya.wait_recv()
        corner_a.append(pass_on(0, 1, 0, 0, x_dev, thirds[1]))
        hand(0, 1, 0, 0)
        fz = NZ - 1 - pz

        def up_arrived(zs):
            for yy in range(2):
                for i in range(2):
                    up_wait(zs, yy, i)

        up_arrived(mz)

        KQ = D // NZ
        near_k = pl.ds(pl.multiple_of(jnp.where(fz == 0, KQ, 0), KQ), D - KQ)
        far_k = pl.ds(pl.multiple_of(fz * KQ, KQ), KQ)

        def handed(s, group):
            for dy, dx in group:
                arrive(hand_first + (s * 2 + dy) * 2 + dx, rows.at[pl.ds(0, 2)])

        def over(group, one):
            first = group[0][0] * 2 + group[0][1]
            lax.fori_loop(first, first + len(group), one, 0)

        def chip(n):
            return (y + n // 2) % 2 * 2 + (x + n % 2) % 2

        def units_of(i):
            return pl.ds(pl.multiple_of(i * 4, 4), 4)

        def up_near(group):
            handed(0, group)

            def one(n, _):
                i = chip(n)
                up_sum[i] = dot(rows[units_of(i), :, near_k].reshape(2 * RT, D - KQ), up_buf[near_k, :])
                return 0

            over(group, one)

        def up_far(group):
            def one(n, _):
                i = chip(n)
                h = up_sum[i] + dot(rows[units_of(i), :, far_k].reshape(2 * RT, KQ), up_buf[far_k, :])
                h = jnp.maximum(h, 0.0)
                hidden[i] = (h * h).astype(BF16)
                return 0

            over(group, one)

        def up_rows(s, group):
            handed(s, group)

            def one(n, _):
                i = s * 4 + chip(n)
                h = jnp.maximum(dot(rows[units_of(i)].reshape(2 * RT, D), up_buf[...]), 0.0)
                hidden[i] = (h * h).astype(BF16)
                return 0

            over(group, one)

        slots = SLOTS

        def plane_of(i):
            if isinstance(i, int):
                return (z, mz, pz, NZ - 1 - pz)[i]
            return jnp.where(i == 0, z, jnp.where(i == 1, mz, jnp.where(i == 2, pz, NZ - 1 - pz)))

        def down_ready(i, yy):
            zs = (z, mz, pz, NZ - 1 - pz)[i]
            for h in range(2):
                down_wait(zs, yy, h)
                if i == 2:
                    relay_of(yy, h).start()

        relay_slots = [[z_slot() for _ in range(2)] for _ in range(2)]

        def relay_of(yy, h):
            ref = down_at(pz, yy, h)
            return z_copy(relay_slots[yy][h], down_sem(pz, yy, h), ref, ref, mz)

        def d_mate(k):
            return copy_of(to_mate + k % slots, part.at[k % slots, :, :, :, 1 - c], mate_in.at[k % slots], mate_dev)

        def d_x(k):
            return copy_of(to_x + k % slots, part.at[k % slots, :, ox, 0, c], x_in.at[k % slots], x_dev)

        def d_y(k):
            return copy_of(to_y + k % slots, part.at[k % slots, oy, :, 1, c], y_in.at[k % slots], y_dev)

        def d_last(k, h):
            src = part.at[k % slots, y, ox, 1, c] if h else part.at[k % slots, oy, x, 0, c]
            return copy_of(to_last + 2 * (k % slots) + h, src, last_in.at[k, h], x_dev if h else y_dev)

        def d_through(k, h):
            src = part.at[k % slots, y, :, 1, c] if h else part.at[k % slots, :, x, 0, c]
            n = chunk_kind(k)[1]
            return copy_of(to_last + 2 * n + h, src, z_in.at[n, h], dev(pz), to_last + 2 * (k % slots) + h)

        def d_done(k):
            m = chunk_kind(k)[1] // 2 - 1
            return copy_of(to_done + m, part.at[k % slots, y, x, :, c], z_done.at[m], dev(pz))

        def split(k, through, other):
            s, n, last = chunk_kind(k)
            if isinstance(k, int):
                (through if s and not last else other)()
            else:
                pl.when((s == 1) & jnp.logical_not(last))(through)
                pl.when((s == 0) | last)(other)

        def sent_all(k):
            d_mate(k).wait_send()
            d_x(k).wait_send()
            d_y(k).wait_send()

            def through():
                for h in range(2):
                    d_through(k, h).wait_send()

            def other():
                for h in range(2):
                    d_last(k, h).wait_send()

            split(k, through, other)

            @pl.when(chunk_kind(k)[2])
            def _():
                d_done(k).wait_send()

        def multiply(k):
            s, i, yy = chunk_at(k)
            j = plane_of(i) * 2 + yy
            got = dot(hidden[pl.ds(s * 4, 4)].reshape(8 * RT, FH), down_buf[j]).astype(BF16)
            part[k % slots] = got.reshape(2, 2, 2, 2, RH, CB)
            d_mate(k).start()

        def fold(k):
            slot = k % slots
            d_mate(k).wait_recv()

            def one(q, _):
                for h in range(2):
                    part[slot, q // 2, q % 2, h, c] = (
                        part[slot, q // 2, q % 2, h, c].astype(F32) + mate_in[slot, q // 2, q % 2, h].astype(F32)
                    ).astype(BF16)
                return 0

            lax.fori_loop(0, 4, one, 0)
            d_x(k).start()
            d_y(k).start()

        def spread(k):
            slot = k % slots
            d_x(k).wait_recv()
            for i in range(2):
                part[slot, i, x, 0, c] = (
                    part[slot, i, x, 0, c].astype(F32) + x_in[slot, i].astype(F32)
                ).astype(BF16)
            split(k, lambda: d_through(k, 0).start(), lambda: d_last(k, 0).start())
            d_y(k).wait_recv()
            for i in range(2):
                part[slot, y, i, 1, c] = (
                    part[slot, y, i, 1, c].astype(F32) + y_in[slot, i].astype(F32)
                ).astype(BF16)
            split(k, lambda: d_through(k, 1).start(), lambda: d_last(k, 1).start())

        def finish(k):
            s, n, last = chunk_kind(k)
            slot = k % slots
            j = plane_of(n // 2) * 2 + n % 2

            @pl.when(s == 0)
            def _():
                for h in range(2):
                    d_last(k, h).wait_recv()
                    put(j, h, part[slot, y, x, h, c], last_in[k, h])
                put_out(j)

            @pl.when(last)
            def _():
                for h in range(2):
                    d_last(k, h).wait_recv()
                    part[slot, y, x, h, c] = (
                        part[slot, y, x, h, c].astype(F32) + last_in[k, h].astype(F32)
                    ).astype(BF16)
                d_done(k).start()

        most = ((0, 0), (0, 1), (1, 0))
        far_corner = ((1, 1),)
        up_near(most)
        ends[0, 1, 1] = z_arrive(1)
        hand(1, 0, 0, 1)
        down_first.wait_recv()
        down_send(z, oy, 0, mz, sent)
        corner_b.wait_recv()
        hand(0, 1, 1, 1)
        for copy in corner_a:
            copy.wait_recv()
        hand(0, 1, 1, 0)
        ends[1, 1, 0] = [z_arrive(2), z_arrive(3)]
        hand(1, 0, 1, 0)
        up_near(far_corner)
        up_arrived(fz)
        up_far(most + far_corner)
        down_last.wait_recv()
        down_send(z, oy, 1, mz, sent)

        def lead(k, _):
            multiply(k)
            return 0

        ends[1, 1, 1] = [z_arrive(4)]
        lax.fori_loop(0, 2, lead, 0)
        up_rows(1, ((0, 0),))
        ends[1, 1, 1].append(z_arrive(5))
        hand(1, 1, 0, 1)
        fold(0)
        fold(1)
        ends[0, 1, 1].wait_recv()
        hand(1, 0, 1, 1)
        ends[1, 0, 0].wait_recv()
        hand(1, 1, 0, 0)
        up_rows(1, ((0, 1), (1, 0)))
        for copy in ends[1, 1, 1]:
            copy.wait_recv()
        hand(1, 1, 1, 1)
        for copy in ends[1, 1, 0]:
            copy.wait_recv()
        hand(1, 1, 1, 0)
        down_ready(1, 0)
        down_ready(1, 1)
        lax.fori_loop(2, 4, lead, 0)
        down_ready(2, 0)
        spread(0)
        up_rows(1, far_corner)
        fold(2)
        spread(1)

        def turn(k, _):
            pl.when(k >= 5)(lambda: finish(k - 5))
            pl.when((k >= 5) & (k < N_CHUNKS + 3))(lambda: spread(k - 3))
            pl.when(k < N_CHUNKS + 1)(lambda: fold(k - 1))
            for at, i, yy in ((6, 2, 1), (12, 3, 0), (13, 3, 1)):
                pl.when(k == at)(lambda i=i, yy=yy: down_ready(i, yy))
            pl.when((k >= slots) & (k < N_CHUNKS))(lambda: sent_all(k - slots))
            pl.when(k < N_CHUNKS)(lambda: multiply(k))
            return 0

        lax.fori_loop(OWN_LEAD, N_CHUNKS + 5, turn, 0)

        def drain(k, _):
            sent_all(k)
            return 0

        lax.fori_loop(N_CHUNKS - slots, N_CHUNKS, drain, 0)
        for yy in range(2):
            for h in range(2):
                relay_of(yy, h).wait_send()
        copy_of(0, rows.at[pl.ds(0, 16)], rows.at[pl.ds(0, 16)], mate_dev, hand_send).wait_send()
        for copy in sent + pending:
            copy.wait_send()
        pending.clear()

    for when, copy in state_sends:
        @pl.when(when)
        def _(copy=copy):
            copy.wait_send()
    for copy in common + z_copies:
        copy.wait_send()
    pltpu.make_async_copy(out, out_at, osem).wait()


def end_finish(one, z_in, last_in, put, put_out, x, y):
    k, n, j, a, b = one
    a.wait_recv()
    put(j, 0, z_in[n, 0, y], last_in[k, 0])
    b.wait_recv()
    put(j, 1, z_in[n, 1, x], last_in[k, 1])
    put_out(j)


def one_kernel(SP, TP, *args):
    (stream, qw, kw, vw, gw, dw, qn, kn, vn, gn, dn, ow, on, gain, up, down) = args
    T = qw.shape[0]
    NB = T // BLOCK
    D = stream.shape[1]
    RT = T // TP
    RH = RT // 2
    FH = up.shape[1] // 2
    CB = down.shape[1]
    offs, starts = turn_tables(SP, T)
    vmem = pl.BlockSpec(memory_space=pltpu.VMEM)
    hbm = pl.BlockSpec(memory_space=pl.ANY)
    heads = qw.shape[1]
    copies = 94
    return pl.pallas_call(
        functools.partial(layer_kernel, SP, TP),
        out_shape=jax.ShapeDtypeStruct((RT, D), BF16),
        in_specs=[vmem] * 9 + [hbm] * 9,
        out_specs=hbm,
        scratch_shapes=[
            pltpu.VMEM((D, FH), BF16),
            pltpu.VMEM((SP, FH, CB), BF16),
            pltpu.VMEM((TP, 256, D), BF16),
            pltpu.VMEM((7, 208, 128), BF16),
            pltpu.VMEM((T, 256), BF16),
            pltpu.VMEM((2, NB, 128, 128), F32),
            pltpu.VMEM((T, 256), F32),
            pltpu.VMEM((T, 256), BF16),
            pltpu.VMEM((TP, RT, 256), BF16),
            pltpu.VMEM((RT, D), BF16),
            pltpu.VMEM((32, RH, D), BF16),
            pltpu.VMEM((8, 2 * RT, FH), BF16),
            pltpu.VMEM((SLOTS, 2, 2, 2, 2, RH, CB), BF16),
            pltpu.VMEM((SLOTS, 2, 2, 2, RH, CB), BF16),
            pltpu.VMEM((SLOTS, 2, RH, CB), BF16),
            pltpu.VMEM((SLOTS, 2, RH, CB), BF16),
            pltpu.VMEM((2 * SP, 2, RH, CB), BF16),
            pltpu.VMEM((SP, 2, 2, RH, CB), BF16),
            pltpu.VMEM((3, 2, RH, CB), BF16),
            pltpu.VMEM((128, 128), F32),
            pltpu.VMEM((4, 2 * RT, FH), F32),
            pltpu.VMEM((RT, D), BF16),
            pltpu.VMEM((T, heads), BF16),
            pltpu.VMEM((T, heads), BF16),
            pltpu.VMEM((T, heads), BF16),
            pltpu.VMEM((T, heads), BF16),
            pltpu.VMEM((RT, D), BF16),
            pltpu.SemaphoreType.DMA((copies,)),
            pltpu.SemaphoreType.DMA((copies,)),
            pltpu.SemaphoreType.DMA((11,)),
            pltpu.SemaphoreType.DMA((22,)),
            pltpu.SemaphoreType.DMA((32,)),
            pltpu.SemaphoreType.DMA((4,)),
            pltpu.SemaphoreType.DMA,
        ],
        compiler_params=pltpu.CompilerParams(
            collective_id=0, has_side_effects=True, vmem_limit_bytes=63 * 1024 * 1024
        ),
    )(kw, vw, kn, vn, dw, dn, jnp.asarray(offs), jnp.asarray(starts), gain,
      stream, qw, qn, gw, gn, ow, on, up, down)


def fits_kernel(SP, TP, args):
    D, FF = args[14].shape
    T = args[1].shape[0] // SP
    return (
        SP == 8 and TP == 4 and D % (SP * 128) == 0 and T % (TP * 32) == 0 and T % BLOCK == 0
        and args[1].shape[1] == TP * 128 and args[6].shape[1] == TP * 128
    )


def solution(mesh):
    in_specs = (
        P(("sp", "tp"), None),
        P("sp", "tp"),
        P("sp", "tp"),
        P("sp", "tp"),
        P("sp", "tp"),
        P("tp", "sp"),
        P("sp", "tp"),
        P("sp", "tp"),
        P("sp", "tp"),
        P("sp", "tp"),
        P("tp", "sp"),
        P("tp", None),
        P("tp", None),
        P(),
        P("sp", "tp"),
        P("tp", "sp"),
    )
    out_specs = P(("sp", "tp"), None)
    SP, TP = mesh.shape["sp"], mesh.shape["tp"]

    def layer(*args):
        body = functools.partial(one_kernel, SP, TP) if fits_kernel(SP, TP, args) else on_device
        return jax.shard_map(
            body, mesh=mesh, in_specs=in_specs, out_specs=out_specs, check_vma=False
        )(*args)

    return layer
```

```python
import functools
import jax
import jax.numpy as jnp
import numpy as np
from jax import lax
from jax.experimental import pallas as pl
from jax.experimental.pallas import tpu as pltpu
from jax.sharding import PartitionSpec as P

HDW = 128
HDN = 64
BLOCK = 128


head_eps = 1e-05
norm_eps = 1e-06
rope_base = 10000.0


def carried_in(shard, axis, join, neutral):
    place = lax.axis_index(axis)
    gathered = jax.tree.map(
        lambda a, kind: lax.all_gather(a.astype(kind), axis),
        shard,
        (jnp.bfloat16, jnp.bfloat16, jnp.bfloat16, jnp.bfloat16),
    )
    state = jax.tree.map(lambda a, e: jnp.zeros_like(a) + jnp.asarray(e, a.dtype), shard, neutral)

    def one(turn, state):
        return join(
            state,
            jax.tree.map(
                lambda a, own: lax.dynamic_index_in_dim(a, turn, 0, False).astype(own.dtype),
                gathered,
                shard,
            ),
        )

    return lax.fori_loop(0, place, one, state)


def rotate(values, places):
    half = values.shape[-1] // 2
    inverse = rope_base ** (-jnp.arange(half, dtype=jnp.float32) / half)
    angles = places[:, None] * inverse[None, :]
    cosine = jnp.cos(angles)[:, None, :]
    sine = jnp.sin(angles)[:, None, :]
    front = values[..., :half]
    back = values[..., half:]
    return jnp.concatenate([front * cosine - back * sine, back * cosine + front * sine], axis=-1)


def block_step(carried, inputs):
    query, keys, values, log_rate = inputs
    running = jnp.cumsum(log_rate, axis=0)
    spread = running[:, None, :] - running[None, :, :]
    length = log_rate.shape[0]
    lower = (jnp.arange(length)[:, None] >= jnp.arange(length)[None, :])[:, :, None]
    factor = jnp.where(lower, jnp.exp(jnp.minimum(spread, 0.0)), 0.0)
    scores = jnp.einsum("thd,shd->tsh", query, keys) * factor
    within = jnp.einsum("tsh,she->the", scores, values)
    across = jnp.einsum("thd,hde->the", query, carried) * jnp.exp(running)[:, :, None]
    tail_decay = jnp.exp(running[-1][None, :] - running)
    updated = jnp.exp(running[-1])[:, None, None] * carried + jnp.einsum(
        "shd,she->hde", keys * tail_decay[:, :, None], values
    )
    return (updated, within + across)


def head_norm(values):
    centre = values - jnp.mean(values, axis=-1, keepdims=True)
    spread = jnp.mean(centre * centre, axis=-1, keepdims=True)
    return centre * lax.rsqrt(spread + head_eps)


def local_group(query, keys, values, log_rate, width, places):
    length = query.shape[0]
    count_of_heads = query.shape[1] // width
    blocks = length // BLOCK

    def split(array):
        return array.astype(jnp.float32).reshape(length, count_of_heads, width)

    query_rot = rotate(split(query), places)
    keys_rot = rotate(split(keys), places) * width ** (-0.5)
    rates = log_rate.T
    carried = jnp.zeros((count_of_heads, width, width), jnp.float32)
    final_state, outputs = lax.scan(
        block_step,
        carried,
        (
            query_rot.reshape(blocks, BLOCK, count_of_heads, width),
            keys_rot.reshape(blocks, BLOCK, count_of_heads, width),
            split(values).reshape(blocks, BLOCK, count_of_heads, width),
            rates.reshape(blocks, BLOCK, count_of_heads),
        ),
    )
    running = jnp.cumsum(rates, axis=0)
    return (
        query_rot,
        outputs.reshape(length, count_of_heads, width),
        final_state,
        jnp.exp(running[-1]),
        running,
    )


def finish_group(query_rot, outputs, incoming, running, gate):
    length = outputs.shape[0]
    outputs = (
        outputs + jnp.einsum("thd,hde->the", query_rot, incoming) * jnp.exp(running)[:, :, None]
    )
    normed = head_norm(outputs).reshape(length, -1)
    return (jax.nn.silu(gate.astype(jnp.float32)) * normed).astype(jnp.bfloat16)


def chain(earlier, later):
    rate_wide, memory_wide, rate_narrow, memory_narrow = earlier
    later_rate_wide, later_memory_wide, later_rate_narrow, later_memory_narrow = later
    return (
        rate_wide * later_rate_wide,
        memory_wide * later_rate_wide[:, None, None] + later_memory_wide,
        rate_narrow * later_rate_narrow,
        memory_narrow * later_rate_narrow[:, None, None] + later_memory_narrow,
    )


def row_norm(middle, norm_gain):
    middle_f = middle.astype(jnp.float32)
    scale = lax.rsqrt(jnp.mean(middle_f * middle_f, axis=-1, keepdims=True) + norm_eps)
    return (middle_f * scale * norm_gain.astype(jnp.float32)).astype(jnp.bfloat16)


def on_device(
    stream_in,
    query_wide,
    key_wide,
    value_wide,
    gate_wide,
    decay_wide,
    query_narrow,
    key_narrow,
    value_narrow,
    gate_narrow,
    decay_narrow,
    output_wide,
    output_narrow,
    norm_gain,
    up_weight,
    down_weight,
):
    length = query_wide.shape[0]
    places = (lax.axis_index("sp") * length + jnp.arange(length, dtype=jnp.int32)).astype(
        jnp.float32
    )
    wide_query, wide_out, wide_state, wide_total, wide_running = local_group(
        query_wide, key_wide, value_wide, decay_wide, HDW, places
    )
    narrow_query, narrow_out, narrow_state, narrow_total, narrow_running = local_group(
        query_narrow, key_narrow, value_narrow, decay_narrow, HDN, places
    )
    identity = (
        jnp.ones_like(wide_total),
        jnp.zeros_like(wide_state),
        jnp.ones_like(narrow_total),
        jnp.zeros_like(narrow_state),
    )
    incoming = carried_in(
        (wide_total, wide_state, narrow_total, narrow_state), "sp", chain, identity
    )
    mixed_wide = finish_group(wide_query, wide_out, incoming[1], wide_running, gate_wide)
    mixed_narrow = finish_group(narrow_query, narrow_out, incoming[3], narrow_running, gate_narrow)
    mixed_sum = lax.psum_scatter(
        (
            jnp.dot(mixed_wide, output_wide, preferred_element_type=jnp.float32)
            + jnp.dot(mixed_narrow, output_narrow, preferred_element_type=jnp.float32)
        ).astype(jnp.bfloat16),
        "tp",
        scatter_dimension=0,
        tiled=True,
    ).astype(jnp.float32)
    middle = (stream_in.astype(jnp.float32) + mixed_sum).astype(jnp.bfloat16)
    normed = lax.all_gather(row_norm(middle, norm_gain), "tp", axis=0, tiled=True)
    up_sum = jnp.dot(
        normed,
        lax.all_gather(up_weight, "sp", axis=0, tiled=True),
        preferred_element_type=jnp.float32,
    )
    hidden = jnp.square(jax.nn.relu(up_sum)).astype(jnp.bfloat16)
    down_sum = jnp.dot(
        hidden,
        lax.all_gather(down_weight, "sp", axis=1, tiled=True),
        preferred_element_type=jnp.float32,
    )
    down_rows = lax.psum_scatter(
        down_sum.astype(jnp.bfloat16), "tp", scatter_dimension=0, tiled=True
    ).astype(jnp.float32)
    return (middle.astype(jnp.float32) + down_rows).astype(jnp.bfloat16)


F32 = jnp.float32
BF16 = jnp.bfloat16
MESH_ID = pl.DeviceIdType.MESH


def turn_tables(shards, length):
    lane = np.arange(128)
    offsets, starts = [], []
    for width in (HDW, HDN):
        half = width // 2
        inverse = rope_base ** (-((lane % half).astype(np.float64)) / half)
        inside = np.arange(BLOCK)[:, None] * inverse[None, :]
        first = (np.arange(shards * length // BLOCK) * BLOCK)[:, None] * inverse[None, :]
        offsets += [np.cos(inside), np.sin(inside)]
        starts += [np.cos(first), np.sin(first)]
    return np.stack(offsets).astype(np.float32), np.stack(starts).astype(np.float32)


def dot(a, b):
    return jnp.dot(a, b, preferred_element_type=F32)


def dot_rows(a, b):
    return lax.dot_general(a, b, (((0,), (0,)), ((), ())), preferred_element_type=F32)


def dot_cols(a, b):
    return lax.dot_general(a, b, (((1,), (1,)), ((), ())), preferred_element_type=F32)


N_CHUNKS = 16
LEAD = 2
SLOTS = 8


ORDER = [0, 1, 8, 9, 2, 10, 11, 12, 13, 3, 14, 4, 5, 15, 6, 7]


def chunk_at(k):
    if isinstance(k, int):
        code = ORDER[k]
    else:
        code = ORDER[0]
        for i, value in enumerate(ORDER[1:], 1):
            code = jnp.where(k == i, value, code)
    n = code % 8
    return code // 8, n // 2, n % 2


def chunk_kind(k):
    s, i, yy = chunk_at(k)
    return s, i * 2 + yy


def layer_kernel(
    SP, TP,
    kw, vw, kn, vn, dw, dn, offs, starts, gain, stream_at, qw_at, qn_at, gw_at, gn_at, ow_w, ow_n, up, down,
    out_at,
    up_buf, down_buf, ow_buf, st_buf, k_rot, before, inside, mixed, mix_in, mid, rows, hidden, part,
    mate_in, x_in, y_in, last_in, z_in, z_done, rates_buf, up_sum, stream, qw, qn, gw, gn, out,
    ssem, rsem, lsem, zsend, zrecv, srecv, osem,
):
    sp = lax.axis_index("sp")
    tp = lax.axis_index("tp")
    NZ = SP // 2
    z, y = sp // 2, sp % 2
    x, c = tp // 2, tp % 2
    T = kw.shape[0]
    NB = T // BLOCK
    RT = T // TP
    RH = RT // 2
    RB = up.shape[0]
    CB = down.shape[1]
    D = up_buf.shape[0]
    FH = up.shape[1] // 2
    heavy = (z == 1) | (z == 2)
    is_end = jnp.logical_not(heavy)
    pz = z + 1 - 2 * (z % 2)
    mz = NZ - 1 - z
    goal_z = jnp.where(heavy, mz, pz)

    def dev(zz, dy=0, dx=0, dc=0):
        return (zz * 2 + (y + dy) % 2, (x + dx) % 2 * 2 + (c + dc) % 2)

    x_dev, y_dev, mate_dev = dev(z, 0, 1), dev(z, 1), dev(z, 0, 0, 1)
    count = [0]
    pending = []

    def link():
        count[0] += 1
        return count[0] - 1

    def copy_of(k, src, dst, device, ks=None):
        return pltpu.make_async_remote_copy(
            src_ref=src, dst_ref=dst, send_sem=ssem.at[k if ks is None else ks], recv_sem=rsem.at[k],
            device_id=device, device_id_type=MESH_ID,
        )

    def start(k, src, dst, device):
        copy = copy_of(k, src, dst, device)
        copy.start()
        pending.append(copy)
        return copy

    def send(src, dst, device):
        return start(link(), src, dst, device)

    def arrive(k, dst):
        copy_of(k, dst, dst, mate_dev).wait_recv()

    locals_ = []

    def keep(src, dst):
        copy = pltpu.make_async_copy(src, dst, lsem.at[len(locals_)])
        copy.start()
        locals_.append(copy)
        return copy

    barrier = pltpu.get_barrier_semaphore()
    for d in range(1, NZ):
        pl.semaphore_signal(barrier, inc=1, device_id=dev((z + d) % NZ), device_id_type=MESH_ID)
    for device in (x_dev, y_dev, mate_dev, dev(z, 0, 1, 1)):
        pl.semaphore_signal(barrier, inc=1, device_id=device, device_id_type=MESH_ID)
    for src, dst in ((qw_at, qw), (qn_at, qn), (gw_at, gw), (gn_at, gn), (stream_at, stream)):
        keep(src, dst)
    pl.semaphore_wait(barrier, NZ + 3)

    HB = RB // 2
    HF = FH // 2

    def up_at(zs, yy, part_of):
        return up_buf.at[pl.ds(pl.multiple_of((zs * 2 + yy) * RB + part_of * HB, HB), HB), :]

    def down_at(zs, yy, part_of):
        return down_buf.at[zs * 2 + yy, pl.ds(part_of * HF, HF), :]

    def up_half(half, part_of):
        return up.at[pl.ds(part_of * HB, HB), pl.ds(pl.multiple_of(half * FH, FH), FH)]

    def down_half(half, part_of):
        return down.at[pl.ds(pl.multiple_of(half * FH + part_of * HF, HF), HF), :]

    z_copies = []

    def z_copy(slot, sem, src, dst, zz):
        return pltpu.make_async_remote_copy(
            src_ref=src, dst_ref=dst, send_sem=zsend.at[slot], recv_sem=zrecv.at[sem],
            device_id=dev(zz), device_id_type=MESH_ID,
        )

    def up_sem(zs, yy, part_of):
        return (zs * 2 + yy) * 2 + part_of

    def down_sem(zs, yy, part_of):
        return 4 * NZ + up_sem(zs, yy, part_of)

    z_slots = [0]

    def z_slot():
        z_slots[0] += 1
        return z_slots[0] - 1

    def up_send(zs, yy, part_of, src, zz, into):
        copy = z_copy(z_slot(), up_sem(zs, yy, part_of), src, up_at(zs, yy, part_of), zz)
        copy.start()
        into.append(copy)

    def down_send(zs, yy, part_of, zz, into):
        ref = down_at(zs, yy, part_of)
        copy = z_copy(z_slot(), down_sem(zs, yy, part_of), ref, ref, zz)
        copy.start()
        into.append(copy)

    def up_wait(zs, yy, part_of):
        ref = up_at(zs, yy, part_of)
        z_copy(0, up_sem(zs, yy, part_of), ref, ref, goal_z).wait_recv()

    def down_wait(zs, yy, part_of):
        ref = down_at(zs, yy, part_of)
        z_copy(0, down_sem(zs, yy, part_of), ref, ref, goal_z).wait_recv()

    oy = 1 - y
    ox = 1 - x
    RW = D * 3 // 8
    QB = HB // 4

    def ow_at(i, g, cols):
        return ow_buf.at[i, pl.ds(g * 128, 128), cols]

    def relay_cols(yy):
        return pl.ds(pl.multiple_of(yy * (D - RW), 128), RW)

    main_cols = pl.ds(RW, D - 2 * RW)
    every = pl.ds(0, D)
    side = ox * 2 + c
    ow_first = [
        send(r.at[:, relay_cols(y)], ow_at(tp, g, relay_cols(y)), x_dev) for g, r in enumerate((ow_w, ow_n))
    ]
    ow_main = [
        send(r.at[:, main_cols], ow_at(tp, g, main_cols), x_dev) for g, r in enumerate((ow_w, ow_n))
    ]
    ow_mate = [send(r, ow_at(tp, g, every), mate_dev) for g, r in enumerate((ow_w, ow_n))]
    up_send(z, y, 0, up_half(y, 0), goal_z, z_copies)
    keep(ow_w, ow_at(tp, 0, every))
    keep(ow_n, ow_at(tp, 1, every))
    keep(up_half(y, 0), up_at(z, y, 0))
    keep(up_half(y, 1), up_at(z, y, 1))
    for i in range(2):
        keep(down_half(y, i), down_at(z, y, i))

    def cross_rows(first, many):
        return send(
            up.at[pl.ds(first, many), pl.ds(pl.multiple_of(oy * FH, FH), FH)],
            up_buf.at[pl.ds(pl.multiple_of(sp * RB + first, QB), many), :], y_dev,
        )

    cross_first = [cross_rows(0, QB)]

    lane = lax.broadcasted_iota(jnp.int32, (128, 128), 1)
    row = lax.broadcasted_iota(jnp.int32, (128, 128), 0)
    lower = row >= lane
    low = lane < HDN
    low_row = row < HDN
    low_half = lax.broadcasted_iota(jnp.int32, (HDN, 128), 1) < HDN
    diagonal = low == low_row
    for h in range(3):
        for b in range(NB):
            ref = dw if h == 0 else dn
            at = 0 if h == 0 else h - 1
            rates_buf[h * NB + b:h * NB + b + 1, :] = ref[at:at + 1, b * BLOCK:(b + 1) * BLOCK]
    cr = rates_buf[...]
    step = 1
    while step < 128:
        cr = cr + jnp.where(lane >= step, pltpu.roll(cr, step, 1), 0.0)
        step *= 2
    ct = cr.T

    def col(h, b):
        return ct[:, h * NB + b:h * NB + b + 1]

    def line(h, b):
        return cr[h * NB + b:h * NB + b + 1, :]

    def total(h, b):
        return cr[h * NB + b:h * NB + b + 1, 127:128]

    def pair(a, b):
        return jnp.where(low, a, b)

    sign_w = jnp.where(low, -1.0, 1.0)
    early = (lane % HDN) < HDN // 2
    sign_n = jnp.where(early, -1.0, 1.0)

    def tables(g, b):
        cb = starts[2 * g, pl.ds(sp * NB + b, 1), :]
        sb = starts[2 * g + 1, pl.ds(sp * NB + b, 1), :]
        co, so = offs[2 * g], offs[2 * g + 1]
        return co * cb - so * sb, (so * cb + co * sb) * (sign_n if g else sign_w)

    def turned(v, table, g):
        if g:
            other = jnp.where(early, pltpu.roll(v, 128 - HDN // 2, 1), pltpu.roll(v, HDN // 2, 1))
        else:
            other = pltpu.roll(v, HDW // 2, 1)
        return v * table[0] + other * table[1]

    state_w = jnp.zeros((128, 128), F32)
    state_n = jnp.zeros((128, 128), F32)
    sums = [jnp.zeros((1, 1), F32) for _ in range(3)]
    for b in range(NB):
        rs = pl.ds(b * BLOCK, BLOCK)
        before[0, b] = state_w
        before[1, b] = state_n
        kwr = turned(kw[rs, :].astype(F32), tables(0, b), 0) * HDW ** (-0.5)
        knr = turned(kn[rs, :].astype(F32), tables(1, b), 1) * HDN ** (-0.5)
        k_rot[rs, 0:128] = kwr.astype(BF16)
        k_rot[rs, 128:256] = knr.astype(BF16)
        t0, t1, t2 = total(0, b), total(1, b), total(2, b)
        sums = [s + t for s, t in zip(sums, (t0, t1, t2))]
        tail_w = jnp.exp(t0 - col(0, b))
        tail_n = pair(jnp.exp(t1 - col(1, b)), jnp.exp(t2 - col(2, b)))
        state_w = jnp.exp(t0) * state_w + dot_rows((kwr * tail_w).astype(BF16), vw[rs, :])
        grown = dot_rows((knr * tail_n).astype(BF16), vn[rs, :])
        state_n = jnp.where(low_row, jnp.exp(t1), jnp.exp(t2)) * state_n + jnp.where(diagonal, grown, 0.0)
    small = lax.broadcasted_iota(jnp.int32, (16, 128), 0)
    rates = jnp.where(small == 0, jnp.exp(sums[0]), jnp.where(small == 1, jnp.exp(sums[1]), jnp.exp(sums[2])))
    st_buf[0, 0:128, :] = state_w.astype(BF16)
    st_buf[0, 128:192, :] = (state_n[0:HDN, :] + state_n[HDN:128, :]).astype(BF16)
    st_buf[0, 192:208, :] = rates.astype(BF16)
    state_y = send(st_buf.at[0], st_buf.at[1], y_dev)
    cross_first.append(cross_rows(QB, HB - QB))

    for copy in locals_[:2]:
        copy.wait()
    for b in range(NB):
        rs = pl.ds(b * BLOCK, BLOCK)
        kwr, knr = k_rot[rs, 0:128], k_rot[rs, 128:256]
        qwr = turned(qw[rs, :].astype(F32), tables(0, b), 0)
        qnr = turned(qn[rs, :].astype(F32), tables(1, b), 1)

        def factor(h):
            return jnp.where(lower, jnp.exp(jnp.minimum(col(h, b) - line(h, b), 0.0)), 0.0)

        scores = (dot_cols(qwr.astype(BF16), kwr) * factor(0)).astype(BF16)
        inside[rs, 0:128] = dot(scores, vw[rs, :])
        near = (dot_cols(jnp.where(low, qnr, 0.0).astype(BF16), knr) * factor(1)).astype(BF16)
        far = (dot_cols(jnp.where(low, 0.0, qnr).astype(BF16), knr) * factor(2)).astype(BF16)
        inside[rs, 128:256] = pair(dot(near, vn[rs, :]), dot(far, vn[rs, :]))
        k_rot[rs, 0:128] = (qwr * jnp.exp(col(0, b))).astype(BF16)
        k_rot[rs, 128:256] = (qnr * pair(jnp.exp(col(1, b)), jnp.exp(col(2, b)))).astype(BF16)

    def state(i):
        return st_buf[i, 0:128, :].astype(F32), st_buf[i, 128:192, :].astype(F32), st_buf[i, 192:208, :].astype(F32)

    def chained(first, second):
        r = second[2]
        return (
            first[0] * r[0:1, :] + second[0],
            first[1] * jnp.where(low_half, r[1:2, :], r[2:3, :]) + second[1],
            first[2] * r,
        )

    state_y.wait_recv()
    mine, theirs = state(0), state(1)
    lead = [jnp.where(y == 0, a, b) for a, b in zip(mine, theirs)]
    rear = [jnp.where(y == 0, b, a) for a, b in zip(mine, theirs)]
    plane = chained(lead, rear)
    st_buf[2, 0:128, :] = plane[0].astype(BF16)
    st_buf[2, 128:192, :] = plane[1].astype(BF16)
    st_buf[2, 192:208, :] = plane[2].astype(BF16)

    def state_copy(k, zs, zz):
        return pltpu.make_async_remote_copy(
            src_ref=st_buf.at[2], dst_ref=st_buf.at[3 + zs], send_sem=ssem.at[k], recv_sem=srecv.at[zs],
            device_id=dev(zz), device_id_type=MESH_ID,
        )

    state_sends = []
    for d in range(NZ - 1, 0, -1):
        copy = state_copy(link(), z, (z + d) % NZ)
        state_sends.append((z + d < NZ, copy))

        @pl.when(z + d < NZ)
        def _(copy=copy):
            copy.start()

    up_send(z, y, 1, up_half(y, 1), goal_z, z_copies)
    ow_y = []
    for g, copy in enumerate(ow_first):
        copy.wait_recv()
        ow_y.append(send(ow_at(side, g, relay_cols(y)), ow_at(side, g, relay_cols(y)), y_dev))
    cross_last = send(up_half(oy, 1), up_at(z, y, 1), y_dev)
    ow_hand = [send(ow_buf.at[side, :, relay_cols(y)], ow_buf.at[side, :, relay_cols(y)], mate_dev)]

    for copy in cross_first:
        copy.wait_recv()
    up_send(z, oy, 0, up_at(z, oy, 0), goal_z, z_copies)
    for zs in range(NZ - 1):
        @pl.when(zs < z)
        def _(zs=zs):
            state_copy(0, zs, mz).wait_recv()

    held = (jnp.zeros((128, 128), F32), jnp.zeros((HDN, 128), F32), jnp.zeros((16, 128), F32))
    for zs in range(NZ - 1):
        held = [jnp.where(zs < z, a, b) for a, b in zip(chained(held, state(3 + zs)), held)]
    held = [jnp.where(y == 1, a, b) for a, b in zip(chained(held, theirs), held)]
    s_w = held[0]
    s_n = jnp.concatenate([jnp.where(low_half, held[1], 0.0), jnp.where(low_half, 0.0, held[1])], axis=0)

    for copy in locals_[2:4]:
        copy.wait()
    sums = [jnp.zeros((1, 1), F32) for _ in range(3)]
    for b in range(NB):
        rs = pl.ds(b * BLOCK, BLOCK)
        whole_w = before[0, b] + jnp.exp(sums[0]) * s_w
        whole_n = before[1, b] + jnp.where(low_row, jnp.exp(sums[1]), jnp.exp(sums[2])) * s_n
        sums = [s + total(h, b) for h, s in enumerate(sums)]
        o_w = inside[rs, 0:128] + dot(k_rot[rs, 0:128], whole_w.astype(BF16))
        o_n = inside[rs, 128:256] + dot(k_rot[rs, 128:256], whole_n.astype(BF16))

        def both(v):
            first = jnp.sum(jnp.where(low, v, 0.0), axis=-1, keepdims=True) / HDN
            second = jnp.sum(jnp.where(low, 0.0, v), axis=-1, keepdims=True) / HDN
            return pair(first, second)

        c_w = o_w - jnp.mean(o_w, axis=-1, keepdims=True)
        n_w = c_w * lax.rsqrt(jnp.mean(c_w * c_w, axis=-1, keepdims=True) + head_eps)
        c_n = o_n - both(o_n)
        n_n = c_n * lax.rsqrt(both(c_n * c_n) + head_eps)
        mixed[rs, 0:128] = (jax.nn.silu(gw[rs, :].astype(F32)) * n_w).astype(BF16)
        mixed[rs, 128:256] = (jax.nn.silu(gn[rs, :].astype(F32)) * n_n).astype(BF16)

    def my_rows(i):
        return pl.ds(pl.multiple_of(i * RT, RT), RT)

    swaps = [
        send(mixed.at[my_rows((x + dx) % 2 * 2 + (c + dc) % 2), :], mix_in.at[tp], dev(z, 0, dx, dc))
        for dx, dc in ((1, 0), (1, 1), (0, 1))
    ]
    mix_in[tp] = mixed[my_rows(tp), :]
    for copy in ow_main:
        copy.wait_recv()
    ow_hand.append(send(ow_buf.at[side, :, main_cols], ow_buf.at[side, :, main_cols], mate_dev))
    for copy in ow_y:
        copy.wait_recv()
    ow_hand.append(send(ow_buf.at[side, :, relay_cols(oy)], ow_buf.at[side, :, relay_cols(oy)], mate_dev))
    for copy in ow_mate + ow_hand + swaps:
        copy.wait_recv()
    for copy in locals_[4:]:
        copy.wait()

    def project(i, _):
        cs = pl.ds(pl.multiple_of(i * 512, 512), 512)
        acc = stream[:, cs].astype(F32)
        for j in range(TP):
            acc = acc + dot(mix_in[j], ow_buf[j, :, cs])
        mid[:, cs] = acc.astype(BF16)
        return 0

    lax.fori_loop(0, D // 512, project, 0)

    own_set = jnp.where(heavy, 0, 1)

    def unit(s, dy, dx, h, dc=0):
        return (((s * 2 + (y + dy) % 2) * 2 + (x + dx) % 2) * 2 + h) * 2 + (c + dc) % 2

    NS = 32

    def norm(i, _):
        m = mid[pl.ds(pl.multiple_of(i * NS, NS), NS), :].astype(F32)
        scale = lax.rsqrt(jnp.mean(m * m, axis=-1, keepdims=True) + norm_eps)
        per = RH // NS
        rows[unit(own_set, 0, 0, i // per), pl.ds(pl.multiple_of(i % per * NS, NS), NS), :] = (
            m * scale * gain[...].reshape(1, D).astype(F32)
        ).astype(BF16)
        return 0

    lax.fori_loop(0, RT // NS, norm, 0)

    def piece(s, dy, dx, h, cut=None):
        if cut is None:
            return rows.at[unit(s, dy, dx, h)]
        return rows.at[unit(s, dy, dx, h), pl.ds(*cut), :]

    def pass_on(s, dy, dx, h, device, cut=None):
        return send(piece(s, dy, dx, h, cut), piece(s, dy, dx, h, cut), device)

    RQ = RH // 2
    whole = (0, RH)
    halves = ((0, RQ), (RQ, RQ))
    thirds = ((0, RH // 3), (RH // 3, RH - RH // 3))
    z_units = [
        (link(), u, cut)
        for u, cuts in (((0, 0, 0), (whole,)), ((0, 0, 1), (whole,)), ((0, 1, 0), halves), ((1, 0, 1), halves))
        for cut in cuts
    ]
    def links(many):
        count[0] += many
        return count[0] - many

    to_mate, to_x, to_y, to_last, to_done = links(SLOTS), links(SLOTS), links(SLOTS), links(2 * SLOTS), link()
    n_done = 3
    ends_of = [k for k in range(N_CHUNKS) if chunk_at(k)[0]]
    common = list(pending)
    pending.clear()

    def cols_of(j):
        return pl.ds(pl.multiple_of(j * CB, CB), CB)

    def put(j, h, *terms):
        rs = pl.ds(h * RH, RH)
        acc = mid[rs, cols_of(j)].astype(F32)
        for term in terms:
            acc = acc + term.astype(F32)
        out[rs, cols_of(j)] = acc.astype(BF16)

    base = count[0]

    def put_out(j):
        pltpu.make_async_copy(out.at[:, cols_of(j)], out_at.at[:, cols_of(j)], osem).start()

    @pl.when(is_end)
    def _():
        sent = []

        def z_unit(i):
            k, (dy, dx, h), cut = z_units[i]
            start(k, piece(1, dy, dx, h, cut), piece(1, dy, dx, h, cut), dev(pz))

        side_x = pass_on(1, 0, 0, 0, x_dev)
        side_y = pass_on(1, 0, 0, 1, y_dev)
        down_first = send(down_half(oy, 0), down_at(z, y, 0), y_dev)
        z_unit(0)
        cross_last.wait_recv()
        up_send(z, oy, 1, up_at(z, oy, 1), goal_z, sent)
        z_unit(1)
        down_last = send(down_half(oy, 1), down_at(z, y, 1), y_dev)
        side_x.wait_recv()
        z_unit(2)
        z_unit(3)
        side_y.wait_recv()
        z_unit(4)
        z_unit(5)
        down_first.wait_recv()
        down_last.wait_recv()
        for yy in range(2):
            for i in range(2):
                down_send(z, yy, i, goal_z, sent)
        order = (pz, NZ - 1 - pz, z, NZ - 1 - z)
        done = []
        for k in ends_of:
            _, n = chunk_kind(k)
            j = order[n // 2] * 2 + n % 2
            if n == n_done:
                continue
            arrive(to_last + 2 * n, z_in.at[n, 0])
            a = send(z_in.at[n, 0, oy], last_in.at[k, 0], y_dev)
            arrive(to_last + 2 * n + 1, z_in.at[n, 1])
            b = send(z_in.at[n, 1, ox], last_in.at[k, 1], x_dev)
            if done:
                end_finish(done[-1], z_in, last_in, put, put_out, x, y)
            done.append((k, n, j, a, b))
        j = order[n_done // 2] * 2 + n_done % 2
        arrive(to_done, z_done)
        for h in range(2):
            put(j, h, z_done[h])
        put_out(j)
        end_finish(done[-1], z_in, last_in, put, put_out, x, y)
        for copy in sent + pending:
            copy.wait_send()
        pending.clear()

    count[0] = base

    @pl.when(heavy)
    def _():
        sent = []
        hand_send = link()
        hand_first = links(8)

        def hand(s, dy, dx, h):
            ref = piece(s, dy, dx, h)
            copy_of(hand_first + (s * 2 + dy) * 2 + dx, ref, ref, mate_dev, hand_send).start()

        def z_arrive(i):
            k, (dy, dx, h), cut = z_units[i]
            arrive(k, piece(1, dy, dx, h, cut))
            return pass_on(1, dy, dx, h, x_dev if h else y_dev, cut)

        def up_relay(yy):
            for i in range(2):
                up_wait(pz, yy, i)
                up_send(pz, yy, i, up_at(pz, yy, i), mz, sent)

        xa = pass_on(0, 0, 0, 0, x_dev)
        yb = pass_on(0, 0, 0, 1, y_dev)
        xb = pass_on(0, 0, 0, 1, x_dev)
        ya = pass_on(0, 0, 0, 0, y_dev)
        down_first = send(down_half(oy, 0), down_at(z, y, 0), y_dev)
        hand(0, 0, 0, 0)
        hand(0, 0, 0, 1)
        cross_last.wait_recv()
        up_send(z, oy, 1, up_at(z, oy, 1), goal_z, sent)
        up_relay(y)
        xa.wait_recv()
        corner_a = [pass_on(0, 0, 1, 0, y_dev, thirds[0])]
        down_last = send(down_half(oy, 1), down_at(z, y, 1), y_dev)
        hand(0, 0, 1, 0)
        yb.wait_recv()
        corner_b = pass_on(0, 1, 0, 1, x_dev)
        hand(0, 1, 0, 1)
        ends = {}
        ends[1, 0, 0] = z_arrive(0)
        hand(1, 0, 0, 0)
        up_relay(oy)
        down_send(z, y, 0, mz, sent)
        down_send(z, y, 1, mz, sent)
        xb.wait_recv()
        hand(0, 0, 1, 1)
        ya.wait_recv()
        corner_a.append(pass_on(0, 1, 0, 0, x_dev, thirds[1]))
        hand(0, 1, 0, 0)
        fz = NZ - 1 - pz

        def up_arrived(zs):
            for yy in range(2):
                for i in range(2):
                    up_wait(zs, yy, i)

        up_arrived(mz)

        KQ = D // NZ
        near_k = pl.ds(pl.multiple_of(jnp.where(fz == 0, KQ, 0), KQ), D - KQ)
        far_k = pl.ds(pl.multiple_of(fz * KQ, KQ), KQ)

        def handed(s, group):
            for dy, dx in group:
                arrive(hand_first + (s * 2 + dy) * 2 + dx, rows.at[pl.ds(0, 2)])

        def over(group, one):
            first = group[0][0] * 2 + group[0][1]
            lax.fori_loop(first, first + len(group), one, 0)

        def chip(n):
            return (y + n // 2) % 2 * 2 + (x + n % 2) % 2

        def units_of(i):
            return pl.ds(pl.multiple_of(i * 4, 4), 4)

        def up_near(group):
            handed(0, group)

            def one(n, _):
                i = chip(n)
                up_sum[i] = dot(rows[units_of(i), :, near_k].reshape(2 * RT, D - KQ), up_buf[near_k, :])
                return 0

            over(group, one)

        def up_far(group):
            def one(n, _):
                i = chip(n)
                h = up_sum[i] + dot(rows[units_of(i), :, far_k].reshape(2 * RT, KQ), up_buf[far_k, :])
                h = jnp.maximum(h, 0.0)
                hidden[i] = (h * h).astype(BF16)
                return 0

            over(group, one)

        def up_rows(s, group):
            handed(s, group)

            def one(n, _):
                i = s * 4 + chip(n)
                h = jnp.maximum(dot(rows[units_of(i)].reshape(2 * RT, D), up_buf[...]), 0.0)
                hidden[i] = (h * h).astype(BF16)
                return 0

            over(group, one)

        slots = SLOTS

        def plane_of(i):
            if isinstance(i, int):
                return (z, mz, pz, NZ - 1 - pz)[i]
            return jnp.where(i == 0, z, jnp.where(i == 1, mz, jnp.where(i == 2, pz, NZ - 1 - pz)))

        def down_ready(i, yy):
            zs = (z, mz, pz, NZ - 1 - pz)[i]
            for h in range(2):
                down_wait(zs, yy, h)
                if i == 2:
                    relay_of(yy, h).start()

        relay_slots = [[z_slot() for _ in range(2)] for _ in range(2)]

        def relay_of(yy, h):
            ref = down_at(pz, yy, h)
            return z_copy(relay_slots[yy][h], down_sem(pz, yy, h), ref, ref, mz)

        def d_mate(k):
            return copy_of(to_mate + k % slots, part.at[k % slots, :, :, :, 1 - c], mate_in.at[k % slots], mate_dev)

        def d_x(k):
            return copy_of(to_x + k % slots, part.at[k % slots, :, ox, 0, c], x_in.at[k % slots], x_dev)

        def d_y(k):
            return copy_of(to_y + k % slots, part.at[k % slots, oy, :, 1, c], y_in.at[k % slots], y_dev)

        def d_last(k, h):
            src = part.at[k % slots, y, ox, 1, c] if h else part.at[k % slots, oy, x, 0, c]
            return copy_of(to_last + 2 * (k % slots) + h, src, last_in.at[k, h], x_dev if h else y_dev)

        def d_through(k, h):
            src = part.at[k % slots, y, :, 1, c] if h else part.at[k % slots, :, x, 0, c]
            n = chunk_kind(k)[1]
            return copy_of(to_last + 2 * n + h, src, z_in.at[n, h], dev(pz), to_last + 2 * (k % slots) + h)

        def d_done(k):
            return copy_of(to_done, part.at[k % slots, y, x, :, c], z_done, dev(pz))

        def split(k, through, other):
            s, n = chunk_kind(k)
            if isinstance(k, int):
                (through if s and n != n_done else other)()
            else:
                pl.when((s == 1) & (n != n_done))(through)
                pl.when((s == 0) | (n == n_done))(other)

        def sent_all(k):
            d_mate(k).wait_send()
            d_x(k).wait_send()
            d_y(k).wait_send()

            def through():
                for h in range(2):
                    d_through(k, h).wait_send()

            def other():
                for h in range(2):
                    d_last(k, h).wait_send()

            split(k, through, other)
            s, n = chunk_kind(k)

            @pl.when((s == 1) & (n == n_done))
            def _():
                d_done(k).wait_send()

        def multiply(k):
            s, i, yy = chunk_at(k)
            j = plane_of(i) * 2 + yy
            got = dot(hidden[pl.ds(s * 4, 4)].reshape(8 * RT, FH), down_buf[j]).astype(BF16)
            part[k % slots] = got.reshape(2, 2, 2, 2, RH, CB)
            d_mate(k).start()

        def fold(k):
            slot = k % slots
            d_mate(k).wait_recv()

            def one(q, _):
                for h in range(2):
                    part[slot, q // 2, q % 2, h, c] = (
                        part[slot, q // 2, q % 2, h, c].astype(F32) + mate_in[slot, q // 2, q % 2, h].astype(F32)
                    ).astype(BF16)
                return 0

            lax.fori_loop(0, 4, one, 0)
            d_x(k).start()
            d_y(k).start()

        def spread(k):
            slot = k % slots
            d_x(k).wait_recv()
            for i in range(2):
                part[slot, i, x, 0, c] = (
                    part[slot, i, x, 0, c].astype(F32) + x_in[slot, i].astype(F32)
                ).astype(BF16)
            split(k, lambda: d_through(k, 0).start(), lambda: d_last(k, 0).start())
            d_y(k).wait_recv()
            for i in range(2):
                part[slot, y, i, 1, c] = (
                    part[slot, y, i, 1, c].astype(F32) + y_in[slot, i].astype(F32)
                ).astype(BF16)
            split(k, lambda: d_through(k, 1).start(), lambda: d_last(k, 1).start())

        def finish(k):
            s, n = chunk_kind(k)
            slot = k % slots
            j = plane_of(n // 2) * 2 + n % 2

            @pl.when(s == 0)
            def _():
                for h in range(2):
                    d_last(k, h).wait_recv()
                    put(j, h, part[slot, y, x, h, c], last_in[k, h])
                put_out(j)

            @pl.when((s == 1) & (n == n_done))
            def _():
                for h in range(2):
                    d_last(k, h).wait_recv()
                    part[slot, y, x, h, c] = (
                        part[slot, y, x, h, c].astype(F32) + last_in[k, h].astype(F32)
                    ).astype(BF16)
                d_done(k).start()

        most = ((0, 0), (0, 1), (1, 0))
        far_corner = ((1, 1),)
        up_near(most)
        ends[0, 1, 1] = z_arrive(1)
        hand(1, 0, 0, 1)
        down_first.wait_recv()
        down_send(z, oy, 0, mz, sent)
        corner_b.wait_recv()
        hand(0, 1, 1, 1)
        for copy in corner_a:
            copy.wait_recv()
        hand(0, 1, 1, 0)
        ends[1, 1, 0] = [z_arrive(2), z_arrive(3)]
        hand(1, 0, 1, 0)
        up_near(far_corner)
        up_arrived(fz)
        up_far(most + far_corner)
        down_last.wait_recv()
        down_send(z, oy, 1, mz, sent)

        def lead(k, _):
            multiply(k)
            return 0

        ends[1, 1, 1] = [z_arrive(4)]
        lax.fori_loop(0, 2, lead, 0)
        up_rows(1, ((0, 0),))
        ends[1, 1, 1].append(z_arrive(5))
        hand(1, 1, 0, 1)
        fold(0)
        fold(1)
        ends[0, 1, 1].wait_recv()
        hand(1, 0, 1, 1)
        ends[1, 0, 0].wait_recv()
        hand(1, 1, 0, 0)
        up_rows(1, ((0, 1), (1, 0)))
        for copy in ends[1, 1, 1]:
            copy.wait_recv()
        hand(1, 1, 1, 1)
        for copy in ends[1, 1, 0]:
            copy.wait_recv()
        hand(1, 1, 1, 0)
        up_rows(1, far_corner)
        spread(0)

        def turn(k, _):
            pl.when(k >= 5)(lambda: finish(k - 5))
            pl.when(k == N_CHUNKS)(lambda: fold(k - 1))
            for at, i, yy in ((3, 2, 0), (4, 1, 0), (4, 1, 1), (8, 2, 1), (10, 3, 0), (13, 3, 1)):
                pl.when(k == at)(lambda i=i, yy=yy: down_ready(i, yy))
            pl.when((k >= slots) & (k < N_CHUNKS))(lambda: sent_all(k - slots))
            pl.when(k < N_CHUNKS)(lambda: multiply(k))
            pl.when((k >= 4) & (k < N_CHUNKS + 3))(lambda: spread(k - 3))
            pl.when((k > LEAD) & (k < N_CHUNKS))(lambda: fold(k - 1))
            return 0

        lax.fori_loop(LEAD, N_CHUNKS + 5, turn, 0)

        def drain(k, _):
            sent_all(k)
            return 0

        lax.fori_loop(N_CHUNKS - slots, N_CHUNKS, drain, 0)
        for yy in range(2):
            for h in range(2):
                relay_of(yy, h).wait_send()
        copy_of(0, rows.at[pl.ds(0, 16)], rows.at[pl.ds(0, 16)], mate_dev, hand_send).wait_send()
        for copy in sent + pending:
            copy.wait_send()
        pending.clear()

    for when, copy in state_sends:
        @pl.when(when)
        def _(copy=copy):
            copy.wait_send()
    for copy in common + z_copies:
        copy.wait_send()
    pltpu.make_async_copy(out, out_at, osem).wait()


def end_finish(one, z_in, last_in, put, put_out, x, y):
    k, n, j, a, b = one
    a.wait_recv()
    put(j, 0, z_in[n, 0, y], last_in[k, 0])
    b.wait_recv()
    put(j, 1, z_in[n, 1, x], last_in[k, 1])
    put_out(j)


def one_kernel(SP, TP, *args):
    (stream, qw, kw, vw, gw, dw, qn, kn, vn, gn, dn, ow, on, gain, up, down) = args
    T = qw.shape[0]
    NB = T // BLOCK
    D = stream.shape[1]
    RT = T // TP
    RH = RT // 2
    FH = up.shape[1] // 2
    CB = down.shape[1]
    offs, starts = turn_tables(SP, T)
    vmem = pl.BlockSpec(memory_space=pltpu.VMEM)
    hbm = pl.BlockSpec(memory_space=pl.ANY)
    heads = qw.shape[1]
    copies = 92
    return pl.pallas_call(
        functools.partial(layer_kernel, SP, TP),
        out_shape=jax.ShapeDtypeStruct((RT, D), BF16),
        in_specs=[vmem] * 9 + [hbm] * 9,
        out_specs=hbm,
        scratch_shapes=[
            pltpu.VMEM((D, FH), BF16),
            pltpu.VMEM((SP, FH, CB), BF16),
            pltpu.VMEM((TP, 256, D), BF16),
            pltpu.VMEM((7, 208, 128), BF16),
            pltpu.VMEM((T, 256), BF16),
            pltpu.VMEM((2, NB, 128, 128), F32),
            pltpu.VMEM((T, 256), F32),
            pltpu.VMEM((T, 256), BF16),
            pltpu.VMEM((TP, RT, 256), BF16),
            pltpu.VMEM((RT, D), BF16),
            pltpu.VMEM((32, RH, D), BF16),
            pltpu.VMEM((8, 2 * RT, FH), BF16),
            pltpu.VMEM((SLOTS, 2, 2, 2, 2, RH, CB), BF16),
            pltpu.VMEM((SLOTS, 2, 2, 2, RH, CB), BF16),
            pltpu.VMEM((SLOTS, 2, RH, CB), BF16),
            pltpu.VMEM((SLOTS, 2, RH, CB), BF16),
            pltpu.VMEM((2 * SP, 2, RH, CB), BF16),
            pltpu.VMEM((SP, 2, 2, RH, CB), BF16),
            pltpu.VMEM((2, RH, CB), BF16),
            pltpu.VMEM((128, 128), F32),
            pltpu.VMEM((4, 2 * RT, FH), F32),
            pltpu.VMEM((RT, D), BF16),
            pltpu.VMEM((T, heads), BF16),
            pltpu.VMEM((T, heads), BF16),
            pltpu.VMEM((T, heads), BF16),
            pltpu.VMEM((T, heads), BF16),
            pltpu.VMEM((RT, D), BF16),
            pltpu.SemaphoreType.DMA((copies,)),
            pltpu.SemaphoreType.DMA((copies,)),
            pltpu.SemaphoreType.DMA((11,)),
            pltpu.SemaphoreType.DMA((22,)),
            pltpu.SemaphoreType.DMA((32,)),
            pltpu.SemaphoreType.DMA((4,)),
            pltpu.SemaphoreType.DMA,
        ],
        compiler_params=pltpu.CompilerParams(
            collective_id=0, has_side_effects=True, vmem_limit_bytes=63 * 1024 * 1024
        ),
    )(kw, vw, kn, vn, dw, dn, jnp.asarray(offs), jnp.asarray(starts), gain,
      stream, qw, qn, gw, gn, ow, on, up, down)


def fits_kernel(SP, TP, args):
    D, FF = args[14].shape
    T = args[1].shape[0] // SP
    return (
        SP == 8 and TP == 4 and D % (SP * 128) == 0 and T % (TP * 32) == 0 and T % BLOCK == 0
        and args[1].shape[1] == TP * 128 and args[6].shape[1] == TP * 128
    )


def solution(mesh):
    in_specs = (
        P(("sp", "tp"), None),
        P("sp", "tp"),
        P("sp", "tp"),
        P("sp", "tp"),
        P("sp", "tp"),
        P("tp", "sp"),
        P("sp", "tp"),
        P("sp", "tp"),
        P("sp", "tp"),
        P("sp", "tp"),
        P("tp", "sp"),
        P("tp", None),
        P("tp", None),
        P(),
        P("sp", "tp"),
        P("tp", "sp"),
    )
    out_specs = P(("sp", "tp"), None)
    SP, TP = mesh.shape["sp"], mesh.shape["tp"]

    def layer(*args):
        body = functools.partial(one_kernel, SP, TP) if fits_kernel(SP, TP, args) else on_device
        return jax.shard_map(
            body, mesh=mesh, in_specs=in_specs, out_specs=out_specs, check_vma=False
        )(*args)

    return layer
```
